32 devices in a mesh: ep: 16 (over z, y, x), tp: 2 (over core).
Axes of the slice: x: 2, y: 2, z: 4, core: 2. Of those that a mesh axis runs over, the one named last changes fastest.
Arguments:
- tokens: bfloat16 [256, 2048], P('ep'), may hold values from -6 to 6
- mix_gain: float32 [2048], replicated, may hold values from 0.1 to 1.9
- query_weight: bfloat16 [2048, 1024], P('ep', 'tp'), may hold values from -0.125 to 0.125
- forget_weight: bfloat16 [2048, 1024], P('ep', 'tp'), may hold values from -0.125 to 0.125
- input_weight: bfloat16 [2048, 1024], P('ep', 'tp'), may hold values from -0.125 to 0.125
- lower_bound: float32 [1024], P('tp'), may hold values from 0 to 0.9
- head_gain: float32 [1024], P('tp'), may hold values from 0.1 to 1.9
- out_weight: bfloat16 [1024, 2048], P('tp', 'ep'), may hold values from -0.1875 to 0.1875
- state: float32 [256, 8, 128, 128], P('ep', 'tp'), may hold values from -4 to 4
- ffn_gain: float32 [2048], replicated, may hold values from 0.1 to 1.9
- route_ids: int32 [256, 2], P('ep'), may hold values from 0 to 7, all different within a row; in each aligned block of 16 rows (0 to 15, 16 to 31, ...) at most 6 rows name the same one
- route_weights: float32 [256, 2], P('ep'), may hold values from 0.25 to 1
- expert_gate: bfloat16 [16, 2048, 2048], P('ep', None, 'tp'), may hold values from -0.125 to 0.125
- expert_up: bfloat16 [16, 2048, 2048], P('ep', None, 'tp'), may hold values from -0.125 to 0.125
- expert_down: bfloat16 [16, 2048, 2048], P('ep', 'tp'), may hold values from -0.09375 to 0.09375
Outputs:
- mixed_out: bfloat16 [256, 2048], P('ep', 'tp')
- new_state: float32 [256, 8, 128, 128], P('ep', 'tp')
The draws below stay inside these ranges and needn't reach their ends.
Inputs may be any that keep to these rules, and one draw needn't show every extreme that they name: `route_ids`: each row names 2 different experts; among the rows of one device no expert is named by more than 6 rows, a bound that some block reaches of them.
All inputs are finite; a program needn't handle non-finite values.
Results may differ from the reference program's by a relative error of at most 0.015.
Values may be sent and summed in bfloat16 or wider, within the bound.
A program may use at most 64 MiB of HBM per device.

```python
import math
import jax
import jax.numpy as jnp
import numpy as np
from jax import lax

D = 2048
HEADS = 8
HEAD_DIM = 128
FF_E = 4096
EXPERTS = 8
TOP = 2
SEQ_DEV = 16
CAP = 6
SEQS = 256
SPAN = 2
N_EP = 16
N_TP = 2


def steps_of(own_key, extent, shards, smallest, high):
    def one(position, shards_of):
        steps = jax.random.uniform(jax.random.fold_in(jax.random.fold_in(own_key, 6), position), (shards_of,), jnp.float32, smallest / len(shards), high / len(shards))
        return jnp.repeat(jnp.exp(steps), extent[position] // shards_of).reshape((-1,) + (1,) * (len(extent) - position - 1))

    level = one(*shards[0])
    for cut in shards[1:]:
        level = level * one(*cut)
    return level


def assign_block(own_key, own, number, rows, count, top, bound, slope):
    ranking = jax.random.permutation(own_key, count)
    packed, ordinary = portions_of(count, rows * top, bound, slope, True), portions_of(count, rows * top, bound, slope, False)
    places = jnp.arange(count)

    def named(tallies, rotation):
        used = int((tallies > 0).sum())
        fixed = max(1, used // 4)
        moved = fixed + (places - fixed + rotation * (used - fixed)) % max(1, count - fixed)
        return jnp.zeros((count,), jnp.int32).at[ranking[jnp.where(places < fixed, places, moved)]].set(jnp.asarray(tallies, jnp.int32))

    tallies = jnp.where(number % 4 == 0, named(packed, number // 4), named(ordinary, number - number // 4 - 1))
    mixed = jax.random.permutation(jax.random.fold_in(own, 3), count)
    giver, receiver = mixed[0:count // 2 * 2:2], mixed[1:count // 2 * 2:2]
    margin = jnp.minimum(tallies[giver] - 1, bound - tallies[receiver]) // 2
    margin = jnp.where((giver == ranking[0]) | (receiver == ranking[0]) | (tallies[receiver] == 0), 0, jnp.maximum(margin, 0))
    moved = jax.random.randint(jax.random.fold_in(own, 4), (count // 2,), 0, 1 << 20) % (margin + 1)
    tallies = tallies.at[giver].add(-moved).at[receiver].add(moved)
    labels = jnp.searchsorted(jnp.cumsum(tallies), jnp.arange(rows * top), side="right").astype(jnp.int32)
    grid = labels.reshape(top, rows).T
    grid = grid[jax.random.permutation(jax.random.fold_in(own, 1), rows)]
    rotation = jax.random.randint(jax.random.fold_in(own, 2), (rows, 1), 0, top)
    return jnp.take_along_axis(grid, (jnp.arange(top)[None, :] + rotation) % top, axis=1)


def portions_of(count, total, reach, slope, full):
    weights = [(1 << 20) // math.isqrt(rank ** slope) + 1 for rank in range(1, count + 1)]
    largest = reach if full else min(reach, max(-(-total // count), total * weights[0] // sum(weights)))
    least = 1 if total - largest >= count - 1 else 0
    counts, rest = [largest] + [least] * (count - 1), total - largest - least * (count - 1)
    while rest > 0:
        movable = [i for i in range(1, count) if counts[i] < largest] or [i for i in range(1, count) if counts[i] < reach]
        mass, budget = sum([weights[i] for i in movable]), rest
        for i in movable:
            extra = min(reach - counts[i], max(1, budget * weights[i] // mass), rest)
            counts[i] = counts[i] + extra
            rest = rest - extra
    return np.array(counts)


def centred(own_key, extent, spread, limit, shards=(), held_as=jnp.bfloat16):
    values = spread * jax.random.normal(own_key, extent, jnp.float32)
    if shards:
        values = values * steps_of(own_key, extent, shards, -0.22, 0.18)
    return jnp.clip(values, -limit, limit).astype(held_as)


def setup_inputs(seed: int = 0) -> dict:
    arg_keys = jax.random.split(jax.random.key(seed), 16)
    tokens = centred(arg_keys[0], (SEQS, D), 1.0, 6.0, ((0, 16),))
    mix_gain = jnp.clip(1.0 + 0.18 * jax.random.normal(arg_keys[1], (D,), jnp.float32), 0.1, 1.9)
    query_weight = centred(arg_keys[2], (D, HEADS * HEAD_DIM), D ** -0.5, 0.125, ((0, 16), (1, 2)))
    forget_weight = centred(arg_keys[3], (D, HEADS * HEAD_DIM), D ** -0.5, 0.125, ((0, 16), (1, 2)))
    input_weight = centred(arg_keys[4], (D, HEADS * HEAD_DIM), D ** -0.5, 0.125, ((0, 16), (1, 2)))
    lower_bound = jnp.clip(0.9 * jax.random.uniform(arg_keys[5], (HEADS * HEAD_DIM,), jnp.float32) ** steps_of(arg_keys[5], (HEADS * HEAD_DIM,), ((0, 2),), -0.2, 0.2), 0.0, 0.9)
    head_gain = jnp.clip(1.0 + 0.18 * jax.random.normal(arg_keys[6], (HEADS * HEAD_DIM,), jnp.float32), 0.1, 1.9)
    out_weight = centred(arg_keys[7], (HEADS * HEAD_DIM, D), (HEADS * HEAD_DIM) ** -0.5, 0.1875, ((0, 2), (1, 16)))
    state = centred(arg_keys[8], (SEQS, HEADS, HEAD_DIM, HEAD_DIM), 0.5, 4.0, ((0, 16), (1, 2)), jnp.float32)
    ffn_gain = jnp.clip(1.0 + 0.18 * jax.random.normal(arg_keys[9], (D,), jnp.float32), 0.1, 1.9)
    route_ids_keys = jax.random.split(jax.random.fold_in(arg_keys[10], 1), SEQS // SEQ_DEV)
    route_ids_turns = jax.random.permutation(jax.random.fold_in(arg_keys[10], 3), SEQS // SEQ_DEV)
    route_ids = jax.vmap(lambda own, number: assign_block(jax.random.fold_in(arg_keys[10], 2), own, number, SEQ_DEV, EXPERTS, TOP, CAP, 2))(route_ids_keys, route_ids_turns).reshape((SEQS, TOP))
    route_weights = jnp.clip(0.25 + 0.75 * jax.random.uniform(arg_keys[11], (SEQS, TOP), jnp.float32) ** steps_of(arg_keys[11], (SEQS, TOP), ((0, 16),), -0.2, 0.2), 0.25, 1.0)
    expert_gate = centred(arg_keys[12], (EXPERTS * SPAN, D, FF_E // SPAN), D ** -0.5, 0.125, ((0, 16), (2, 2)))
    expert_up = centred(arg_keys[13], (EXPERTS * SPAN, D, FF_E // SPAN), D ** -0.5, 0.125, ((0, 16), (2, 2)))
    expert_down = centred(arg_keys[14], (EXPERTS * SPAN, FF_E // SPAN, D), FF_E ** -0.5, 0.09375, ((0, 16), (1, 2)))
    return {"tokens": tokens, "mix_gain": mix_gain, "query_weight": query_weight, "forget_weight": forget_weight, "input_weight": input_weight, "lower_bound": lower_bound, "head_gain": head_gain, "out_weight": out_weight, "state": state, "ffn_gain": ffn_gain, "route_ids": route_ids, "route_weights": route_weights, "expert_gate": expert_gate, "expert_up": expert_up, "expert_down": expert_down}


epsilon = 1e-06

def rms_scale(values_in, gain_vec):
    return values_in * lax.rsqrt(lax.optimization_barrier(jnp.mean(values_in * values_in, axis=-1, keepdims=True)) + epsilon) * gain_vec

def reference(tokens, mix_gain, query_weight, forget_weight, input_weight, lower_bound, head_gain, out_weight, state, ffn_gain, route_ids, route_weights, expert_gate, expert_up, expert_down):
    batch_size = tokens.shape[0]
    residual = tokens.astype(jnp.float32)
    normed = rms_scale(residual, mix_gain).astype(jnp.bfloat16)
    queries = jnp.dot(normed, query_weight, preferred_element_type=jnp.float32).reshape(batch_size, HEADS, HEAD_DIM)
    forget_pre = jnp.dot(normed, forget_weight, preferred_element_type=jnp.float32)
    fresh_values = jnp.dot(normed, input_weight, preferred_element_type=jnp.float32).reshape(batch_size, HEADS, HEAD_DIM)
    forget = (lower_bound + (1.0 - lower_bound) * jax.nn.sigmoid(forget_pre)).reshape(batch_size, HEADS, HEAD_DIM)
    new_state = forget[..., None] * state + (1.0 - forget)[..., None] * fresh_values[:, :, None, :]
    readout = jnp.einsum('shk,shkv->shv', queries, new_state, precision=lax.Precision.HIGHEST)
    readout = rms_scale(readout, head_gain.reshape(HEADS, HEAD_DIM))
    heads_out = readout.reshape(batch_size, HEADS * HEAD_DIM).astype(jnp.bfloat16)
    group_cols = HEADS * HEAD_DIM // N_TP
    mixer_sum = jnp.zeros((batch_size, D), jnp.float32)
    for group in range(N_TP):
        product = jnp.dot(heads_out[:, group * group_cols:(group + 1) * group_cols], out_weight[group * group_cols:(group + 1) * group_cols], preferred_element_type=jnp.float32).astype(jnp.bfloat16)
        product = lax.optimization_barrier(product)
        mixer_sum = mixer_sum + product.astype(jnp.float32)
    after_mixer = (residual + mixer_sum).astype(jnp.bfloat16)
    ffn_in = rms_scale(after_mixer.astype(jnp.float32), ffn_gain).astype(jnp.bfloat16)
    expert_span = N_EP // EXPERTS
    span_cols = FF_E // expert_span
    gate_full = expert_gate.reshape(EXPERTS, expert_span, D, span_cols).transpose(0, 2, 1, 3).reshape(EXPERTS, D, FF_E)
    up_full = expert_up.reshape(EXPERTS, expert_span, D, span_cols).transpose(0, 2, 1, 3).reshape(EXPERTS, D, FF_E)
    down_full = expert_down.reshape(EXPERTS, FF_E, D)
    pair_count = SEQ_DEV * TOP
    flat_ids = route_ids.reshape(N_EP, pair_count).astype(jnp.int32)
    onehot = (flat_ids[..., None] == jnp.arange(EXPERTS, dtype=jnp.int32)).astype(jnp.int32)
    slot_rank = lax.optimization_barrier(jnp.sum((jnp.cumsum(onehot, axis=1).astype(jnp.int32) - onehot) * onehot, axis=-1)).astype(jnp.int32)
    slot_index = (jnp.arange(N_EP, dtype=jnp.int32)[:, None] * CAP + slot_rank).reshape(-1).astype(jnp.int32)
    expert_index = flat_ids.reshape(-1)
    token_index = (jnp.arange(batch_size * TOP, dtype=jnp.int32) // TOP).astype(jnp.int32)
    slot_table = jnp.full((EXPERTS, N_EP * CAP), batch_size, dtype=jnp.int32).at[expert_index, slot_index].set(token_index)
    padded_rows = jnp.concatenate([ffn_in, jnp.zeros((1, D), jnp.bfloat16)], axis=0)

    def expert_step(inputs):
        gate_w, up_w, down_w, table_row = inputs
        slot_rows = padded_rows[table_row]
        gate_pre = jnp.dot(slot_rows, gate_w, preferred_element_type=jnp.float32)
        up_pre = jnp.dot(slot_rows, up_w, preferred_element_type=jnp.float32)
        hidden = (jax.nn.silu(gate_pre) * up_pre).astype(jnp.bfloat16)
        return jnp.dot(hidden, down_w, preferred_element_type=jnp.float32)
    expert_out = lax.map(expert_step, (gate_full, up_full, down_full, slot_table))
    picked = expert_out[expert_index, slot_index].reshape(batch_size, TOP, D)
    expert_mix = lax.optimization_barrier(jnp.sum(picked * route_weights[:, :, None], axis=1))
    mixed_out = (after_mixer.astype(jnp.float32) + expert_mix).astype(jnp.bfloat16)
    return (mixed_out, new_state)
```

```python
import functools

import jax
import jax.numpy as jnp
from jax import lax
from jax.experimental import pallas as pl
from jax.experimental.pallas import tpu as pltpu
from jax.sharding import PartitionSpec as P

MESH = pl.DeviceIdType.MESH
EXPERTS = 8
TOP = 2


epsilon = 1e-06


def rms_scale(values_in, gain_vec):
    return (
        values_in
        * lax.rsqrt(jnp.mean(values_in * values_in, axis=-1, keepdims=True) + epsilon)
        * gain_vec
    )


def slot_ranks(block_ids, expert_count):
    onehot = (block_ids[..., None] == jnp.arange(expert_count, dtype=jnp.int32)).astype(jnp.int32)
    before = jnp.cumsum(onehot, axis=1) - onehot
    return jnp.sum(before * onehot, axis=-1)


def gathered_shards(
    tokens,
    mix_gain,
    query_weight,
    forget_weight,
    input_weight,
    lower_bound,
    head_gain,
    out_weight,
    state,
    ffn_gain,
    route_ids,
    route_weights,
    expert_gate,
    expert_up,
    expert_down,
):
    seq_dev = tokens.shape[0]
    model_width = tokens.shape[1]
    ep_count = lax.axis_size("ep")
    residual = tokens.astype(jnp.float32)
    normed = rms_scale(residual, mix_gain).astype(jnp.bfloat16)
    head_count = state.shape[1]
    head_size = state.shape[2]
    proj_width = query_weight.shape[1]
    pieces = (
        lax.all_gather(query_weight, "ep", axis=0, tiled=True),
        lax.all_gather(forget_weight, "ep", axis=0, tiled=True),
        lax.all_gather(input_weight, "ep", axis=0, tiled=True),
    )
    queries, forget_pre, fresh_values = tuple(
        (jnp.dot(normed, weight_rows, preferred_element_type=jnp.float32) for weight_rows in pieces)
    )
    forget = (lower_bound + (1.0 - lower_bound) * jax.nn.sigmoid(forget_pre)).reshape(
        seq_dev, head_count, head_size
    )
    queries = queries.reshape(seq_dev, head_count, head_size)
    fresh_values = fresh_values.reshape(seq_dev, head_count, head_size)
    new_state = forget[..., None] * state + (1.0 - forget)[..., None] * fresh_values[:, :, None, :]
    readout = jnp.einsum("shk,shkv->shv", queries, new_state, precision=lax.Precision.HIGHEST)
    readout = rms_scale(readout, head_gain.reshape(head_count, head_size))
    heads_out = readout.reshape(seq_dev, proj_width).astype(jnp.bfloat16)
    partial_mix = jnp.dot(
        heads_out,
        lax.all_gather(out_weight, "ep", axis=1, tiled=True),
        preferred_element_type=jnp.float32,
    )
    mixer_sum = lax.psum(partial_mix.astype(jnp.bfloat16), "tp").astype(jnp.float32)
    after_mixer = (residual + mixer_sum).astype(jnp.bfloat16)
    ffn_in = rms_scale(after_mixer.astype(jnp.float32), ffn_gain).astype(jnp.bfloat16)
    capacity = 3 * seq_dev // 8
    expert_span = ep_count // EXPERTS
    half_width = model_width // lax.axis_size("tp")
    own_columns = lax.dynamic_slice_in_dim(
        after_mixer, lax.axis_index("tp") * half_width, half_width, 1
    ).astype(jnp.float32)
    gate_slice = expert_gate[0]
    up_slice = expert_up[0]
    down_slice = expert_down[0]
    slot_iota = jnp.arange(capacity, dtype=jnp.int32)
    own_rank = slot_ranks(route_ids.reshape(1, seq_dev * TOP), EXPERTS).reshape(seq_dev, TOP)
    expert_iota = jnp.arange(EXPERTS, dtype=jnp.int32)
    chosen = (route_ids[:, :, None, None] == expert_iota[None, None, :, None]) & (
        own_rank[:, :, None, None] == slot_iota[None, None, None, :]
    )
    dispatch = jnp.any(chosen, axis=1).astype(jnp.bfloat16)
    combine = jnp.sum(chosen.astype(jnp.float32) * route_weights[:, :, None, None], axis=1)
    outgoing = jnp.einsum(
        "tec,td->ecd", dispatch, ffn_in, preferred_element_type=jnp.float32
    ).astype(jnp.bfloat16)
    outgoing = jnp.broadcast_to(
        outgoing[:, None], (EXPERTS, expert_span, capacity, model_width)
    ).reshape(ep_count, capacity, model_width)
    slot_rows = lax.all_to_all(outgoing, "ep", split_axis=0, concat_axis=0, tiled=True)
    gate_pre = jnp.einsum(
        "...d,df->...f", slot_rows, gate_slice, preferred_element_type=jnp.float32
    )
    up_pre = jnp.einsum("...d,df->...f", slot_rows, up_slice, preferred_element_type=jnp.float32)
    hidden = (jax.nn.silu(gate_pre) * up_pre).astype(jnp.bfloat16)
    partial_out = jnp.einsum(
        "...f,fd->...d", hidden, down_slice, preferred_element_type=jnp.float32
    )
    reduced = lax.psum_scatter(
        partial_out.astype(jnp.bfloat16), "tp", scatter_dimension=2, tiled=True
    ).astype(jnp.float32)
    returned = lax.all_to_all(
        reduced.astype(jnp.bfloat16), "ep", split_axis=0, concat_axis=0, tiled=True
    ).astype(reduced.dtype)
    expert_out = jnp.sum(returned.reshape(EXPERTS, expert_span, capacity, half_width), axis=1)
    expert_mix = jnp.einsum("tec,ecd->td", combine, expert_out, precision=lax.Precision.HIGHEST)
    mixed_out = (own_columns + expert_mix).astype(jnp.bfloat16)
    return (mixed_out, new_state)


def layer_kernel(
    n,
    m,
    capacity,
    tokens_ref,
    mix_gain_ref,
    query_ref,
    forget_ref,
    input_ref,
    bound_ref,
    head_gain_ref,
    out_ref,
    state_hbm,
    ffn_gain_ref,
    ids_ref,
    weights_ref,
    gate_hbm,
    up_hbm,
    down_hbm,
    mixed_ref,
    forget_out_ref,
    fresh_out_ref,
    state_buf,
    gate_buf,
    up_buf,
    down_buf,
    x_send,
    x_recv,
    p_send,
    p_recv,
    h_send,
    h_recv,
    m_send,
    m_recv,
    after_buf,
    o_send,
    o_recv,
    hidden_buf,
    r_send,
    r_recv,
    local_sem,
    send_sem,
    recv_sem,
):
    me = lax.axis_index("ep")
    core = lax.axis_index("tp")
    f32, bf16 = jnp.float32, jnp.bfloat16
    seqs, width = tokens_ref.shape
    rows = query_ref.shape[0]
    proj = query_ref.shape[1]
    heads = state_buf.shape[1]
    size = state_buf.shape[2]
    span = n // EXPERTS
    half = width // m

    loads = [
        pltpu.make_async_copy(state_hbm, state_buf, local_sem.at[0]),
        pltpu.make_async_copy(gate_hbm.at[0], gate_buf, local_sem.at[1]),
        pltpu.make_async_copy(up_hbm.at[0], up_buf, local_sem.at[2]),
        pltpu.make_async_copy(down_hbm.at[0], down_buf, local_sem.at[3]),
    ]
    for load in loads:
        load.start()

    barrier = pltpu.get_barrier_semaphore()
    for shift in range(m):
        other = lax.rem(core + shift, m)

        def greet(i, carry, other=other):
            pl.semaphore_signal(
                barrier, inc=1, device_id=(lax.rem(me + i, n), other), device_id_type=MESH
            )
            return carry

        lax.fori_loop(0 if shift else 1, n, greet, 0)

    def copy_to(phase, i, shift, source, target):
        peer = lax.rem(me + i, n)
        other = lax.rem(core + shift, m)
        return pltpu.make_async_remote_copy(
            src_ref=source(peer, other),
            dst_ref=target(me, core),
            send_sem=send_sem.at[phase * m + shift, peer],
            recv_sem=recv_sem.at[phase * m + core, me],
            device_id=(peer, other),
            device_id_type=MESH,
        )

    def copy_from(phase, i, shift, target):
        peer = lax.rem(me - i + n, n)
        other = lax.rem(core - shift + m, m)
        landing = target(peer, other)
        return peer, other, pltpu.make_async_remote_copy(
            src_ref=landing,
            dst_ref=landing,
            send_sem=send_sem.at[phase * m + shift, peer],
            recv_sem=recv_sem.at[phase * m + other, peer],
            device_id=(lax.rem(me + i, n), lax.rem(core + shift, m)),
            device_id_type=MESH,
        )

    def send_all(phase, shift, source, target):
        def step(i, carry):
            copy_to(phase, i, shift, source, target).start()
            return carry

        lax.fori_loop(0 if shift else 1, n, step, 0)

    def receive_all(phase, shift, target):
        def step(i, carry):
            copy_from(phase, i, shift, target)[2].wait_recv()
            return carry

        lax.fori_loop(0 if shift else 1, n, step, 0)

    def drain(phase, shift, source, target):
        def step(i, carry):
            copy_to(phase, i, shift, source, target).wait_send()
            return carry

        lax.fori_loop(0 if shift else 1, n, step, 0)

    residual = tokens_ref[...].astype(f32)
    normed = rms_scale(residual, mix_gain_ref[...]).astype(bf16)
    for peer in range(n):
        x_send[peer] = normed[:, peer * rows : (peer + 1) * rows]

    ids = ids_ref[...]
    routed = weights_ref[...]
    slots = EXPERTS * 8
    lane = lax.broadcasted_iota(jnp.int32, (seqs, slots), 1)
    lane_expert = lane // 8
    lane_slot = lane % 8
    first = jnp.where(lane_expert == ids[:, 0:1], 1.0, 0.0)
    second = jnp.where(lane_expert == ids[:, 1:2], 1.0, 0.0)
    named = first + second
    lower = jnp.where(
        lax.broadcasted_iota(jnp.int32, (seqs, seqs), 1)
        < lax.broadcasted_iota(jnp.int32, (seqs, seqs), 0),
        1.0,
        0.0,
    )
    before = jnp.dot(lower.astype(bf16), named.astype(bf16), preferred_element_type=f32)
    taken = jnp.where(jnp.abs(before - lane_slot.astype(f32)) < 0.5, named, 0.0)
    combine = taken * (first * routed[:, 0:1] + second * routed[:, 1:2])

    pl.semaphore_wait(barrier, n * m - 1)

    x_source, x_target = lambda p, c: x_send.at[p], lambda p, c: x_recv.at[p]
    send_all(0, 0, x_source, x_target)
    x_recv[pl.ds(me, 1)] = x_send[pl.ds(me, 1)]
    receive_all(0, 0, x_target)

    gathered = x_recv[...].reshape(n * seqs, rows)
    for part, ref in enumerate((query_ref, forget_ref, input_ref)):
        p_send[:, :, part * proj : (part + 1) * proj] = (
            jnp.dot(gathered, ref[...], preferred_element_type=f32)
            .reshape(n, seqs, proj)
            .astype(bf16)
        )
    p_source, p_target = lambda p, c: p_send.at[p], lambda p, c: p_recv.at[p]
    send_all(1, 0, p_source, p_target)

    def add_part(i, total):
        peer, _, copy = copy_from(1, i, 0, p_target)
        copy.wait_recv()
        return total + p_recv[peer].astype(f32)

    total = lax.fori_loop(1, n, add_part, p_send[me].astype(f32))
    queries = total[:, :proj]
    bound = bound_ref[...]
    forget = bound + (1.0 - bound) * jax.nn.sigmoid(total[:, proj : 2 * proj])
    fresh = total[:, 2 * proj :]
    forget_out_ref[...] = forget
    fresh_out_ref[...] = fresh

    loads[0].wait()
    scaled = (queries * forget).astype(bf16)
    rest = queries * (1.0 - forget)
    row_of = lax.broadcasted_iota(jnp.int32, (seqs, size), 0)

    def read_row(s, sums):
        return tuple(
            jnp.where(
                row_of == s,
                jnp.dot(
                    scaled[:, h * size : (h + 1) * size],
                    state_buf[s, h].astype(bf16),
                    preferred_element_type=f32,
                ),
                sums[h],
            )
            for h in range(heads)
        )

    sums = lax.fori_loop(
        0, seqs, read_row, tuple(jnp.zeros((seqs, size), f32) for _ in range(heads)), unroll=4
    )
    for h in range(heads):
        cut = slice(h * size, (h + 1) * size)
        readout = sums[h] + jnp.sum(rest[:, cut], axis=-1, keepdims=True) * fresh[:, cut]
        h_send[:, cut] = rms_scale(readout, head_gain_ref[:, cut]).astype(bf16)

    h_source, h_target = lambda p, c: h_send, lambda p, c: h_recv.at[p]
    send_all(2, 0, h_source, h_target)
    h_recv[pl.ds(me, 1)] = h_send[...][None]
    receive_all(2, 0, h_target)
    m_send[...] = (
        jnp.dot(h_recv[...].reshape(n * seqs, proj), out_ref[...], preferred_element_type=f32)
        .reshape(n, seqs, rows)
        .astype(bf16)
    )
    m_source, m_target = lambda p, c: m_send.at[p], lambda p, c: m_recv.at[c, p]
    for shift in range(m):
        send_all(3, shift, m_source, m_target)
    m_recv[pl.ds(core, 1), pl.ds(me, 1)] = m_send[pl.ds(me, 1)][None]
    for shift in range(m):
        receive_all(3, shift, m_target)
    mixer_sum = jnp.concatenate(
        [sum(m_recv[c, p].astype(f32) for c in range(m)) for p in range(n)], axis=1
    )
    after = (residual + mixer_sum).astype(bf16).astype(f32)
    after_buf[...] = after
    ffn_in = rms_scale(after, ffn_gain_ref[...]).astype(bf16)
    o_send[...] = (
        lax.dot_general(
            taken.astype(bf16), ffn_in, (((0,), (0,)), ((), ())), preferred_element_type=f32
        )
        .reshape(EXPERTS, 8, width)
        .astype(bf16)
    )
    o_source, o_target = lambda p, c: o_send.at[lax.div(p, span)], lambda p, c: o_recv.at[p]
    send_all(4, 0, o_source, o_target)
    o_recv[pl.ds(me, 1)] = o_send[pl.ds(lax.div(me, span), 1)]
    receive_all(4, 0, o_target)

    for load in loads[1:]:
        load.wait()
    slot_rows = o_recv[...].astype(f32).reshape(n * 8, width).astype(bf16)
    tile = 256

    def hidden_step(j, carry):
        cut = pl.ds(pl.multiple_of(j * tile, tile), tile)
        gate_pre = jnp.dot(slot_rows, gate_buf[:, cut], preferred_element_type=f32)
        up_pre = jnp.dot(slot_rows, up_buf[:, cut], preferred_element_type=f32)
        hidden_buf[:, cut] = (jax.nn.silu(gate_pre) * up_pre).astype(bf16)
        return carry

    lax.fori_loop(0, gate_buf.shape[1] // tile, hidden_step, 0)
    hidden = hidden_buf[...]
    r_source, r_target = lambda p, c: r_send.at[c, p], lambda p, c: r_recv.at[c, p]
    for shift in reversed(range(m)):
        side = lax.rem(core + shift, m)

        def down_step(j, carry, side=side):
            cut = pl.ds(pl.multiple_of(j * tile, tile), tile)
            taken_cut = pl.ds(pl.multiple_of(side * half + j * tile, tile), tile)
            r_send[side, :, :, cut] = (
                jnp.dot(hidden, down_buf[:, taken_cut], preferred_element_type=f32)
                .reshape(n, 8, tile)
                .astype(bf16)
            )
            return carry

        lax.fori_loop(0, half // tile, down_step, 0)
        send_all(5, shift, r_source, r_target)
    r_recv[pl.ds(core, 1), pl.ds(me, 1)] = r_send[pl.ds(core, 1), pl.ds(me, 1)]
    for shift in reversed(range(m)):
        receive_all(5, shift, r_target)
    expert_out = jnp.concatenate(
        [
            sum(
                r_recv[c, e * span + k].astype(f32) for c in range(m) for k in range(span)
            )
            for e in range(EXPERTS)
        ],
        axis=0,
    )
    expert_mix = jnp.dot(
        combine, expert_out, preferred_element_type=f32, precision=lax.Precision.HIGHEST
    )
    own = after_buf[:, pl.ds(pl.multiple_of(core * half, 128), half)]
    mixed_ref[...] = (own + expert_mix).astype(bf16)

    drain(0, 0, x_source, x_target)
    drain(1, 0, p_source, p_target)
    drain(2, 0, h_source, h_target)
    drain(4, 0, o_source, o_target)
    for shift in range(m):
        drain(3, shift, m_source, m_target)
        drain(5, shift, r_source, r_target)


def exchanged_shards(
    n,
    m,
    tokens,
    mix_gain,
    query_weight,
    forget_weight,
    input_weight,
    lower_bound,
    head_gain,
    out_weight,
    state,
    ffn_gain,
    route_ids,
    route_weights,
    expert_gate,
    expert_up,
    expert_down,
):
    seqs, width = tokens.shape
    rows, proj = query_weight.shape
    heads, size = state.shape[1], state.shape[2]
    columns = out_weight.shape[1]
    hidden = expert_gate.shape[2]
    half = width // m
    f32, bf16 = jnp.float32, jnp.bfloat16
    vmem, far = pl.BlockSpec(memory_space=pltpu.VMEM), pl.BlockSpec(memory_space=pl.ANY)
    mixed_out, forget, fresh = pl.pallas_call(
        functools.partial(layer_kernel, n, m, 3 * seqs // 8),
        out_shape=(
            jax.ShapeDtypeStruct((seqs, half), bf16),
            jax.ShapeDtypeStruct((seqs, proj), f32),
            jax.ShapeDtypeStruct((seqs, proj), f32),
        ),
        in_specs=[vmem] * 8 + [far] + [vmem] * 3 + [far] * 3,
        out_specs=(vmem, vmem, vmem),
        scratch_shapes=[
            pltpu.VMEM(state.shape, f32),
            pltpu.VMEM(expert_gate.shape[1:], bf16),
            pltpu.VMEM(expert_up.shape[1:], bf16),
            pltpu.VMEM(expert_down.shape[1:], bf16),
            pltpu.VMEM((n, seqs, rows), bf16),
            pltpu.VMEM((n, seqs, rows), bf16),
            pltpu.VMEM((n, seqs, 3 * proj), bf16),
            pltpu.VMEM((n, seqs, 3 * proj), bf16),
            pltpu.VMEM((seqs, proj), bf16),
            pltpu.VMEM((n, seqs, proj), bf16),
            pltpu.VMEM((n, seqs, columns), bf16),
            pltpu.VMEM((m, n, seqs, columns), bf16),
            pltpu.VMEM((seqs, width), f32),
            pltpu.VMEM((EXPERTS, 8, width), bf16),
            pltpu.VMEM((n, 8, width), bf16),
            pltpu.VMEM((n * 8, hidden), bf16),
            pltpu.VMEM((m, n, 8, half), bf16),
            pltpu.VMEM((m, n, 8, half), bf16),
            pltpu.SemaphoreType.DMA((4,)),
            pltpu.SemaphoreType.DMA((6 * m, n)),
            pltpu.SemaphoreType.DMA((6 * m, n)),
        ],
        compiler_params=pltpu.CompilerParams(
            collective_id=0, has_side_effects=True, vmem_limit_bytes=60000 * 1024
        ),
    )(
        tokens,
        mix_gain[None],
        query_weight,
        forget_weight,
        input_weight,
        lower_bound[None],
        head_gain[None],
        out_weight,
        state,
        ffn_gain[None],
        route_ids,
        route_weights,
        expert_gate,
        expert_up,
        expert_down,
    )
    forget = forget.reshape(seqs, heads, size)
    fresh = fresh.reshape(seqs, heads, size)
    new_state = forget[..., None] * state + (1.0 - forget)[..., None] * fresh[:, :, None, :]
    return (mixed_out, new_state)


def solution(mesh):
    n, m = mesh.shape["ep"], mesh.shape["tp"]

    def body(*args):
        rows = args[2].shape[0]
        columns = args[7].shape[1]
        if rows % 128 or columns % 128:
            return gathered_shards(*args)
        return exchanged_shards(n, m, *args)

    return jax.shard_map(
        body,
        mesh=mesh,
        in_specs=(
            P("ep", None),
            P(),
            P("ep", "tp"),
            P("ep", "tp"),
            P("ep", "tp"),
            P("tp"),
            P("tp"),
            P("tp", "ep"),
            P("ep", "tp", None, None),
            P(),
            P("ep", None),
            P("ep", None),
            P("ep", None, "tp"),
            P("ep", None, "tp"),
            P("ep", "tp", None),
        ),
        out_specs=(P("ep", "tp"), P("ep", "tp", None, None)),
        check_vma=False,
    )
```

```python
import functools

import jax
import jax.numpy as jnp
from jax import lax
from jax.experimental import pallas as pl
from jax.experimental.pallas import tpu as pltpu
from jax.sharding import PartitionSpec as P

MESH = pl.DeviceIdType.MESH
EXPERTS = 8
TOP = 2


epsilon = 1e-06


def rms_scale(values_in, gain_vec):
    return (
        values_in
        * lax.rsqrt(jnp.mean(values_in * values_in, axis=-1, keepdims=True) + epsilon)
        * gain_vec
    )


def slot_ranks(block_ids, expert_count):
    onehot = (block_ids[..., None] == jnp.arange(expert_count, dtype=jnp.int32)).astype(jnp.int32)
    before = jnp.cumsum(onehot, axis=1) - onehot
    return jnp.sum(before * onehot, axis=-1)


def gathered_shards(
    tokens,
    mix_gain,
    query_weight,
    forget_weight,
    input_weight,
    lower_bound,
    head_gain,
    out_weight,
    state,
    ffn_gain,
    route_ids,
    route_weights,
    expert_gate,
    expert_up,
    expert_down,
):
    seq_dev = tokens.shape[0]
    model_width = tokens.shape[1]
    ep_count = lax.axis_size("ep")
    residual = tokens.astype(jnp.float32)
    normed = rms_scale(residual, mix_gain).astype(jnp.bfloat16)
    head_count = state.shape[1]
    head_size = state.shape[2]
    proj_width = query_weight.shape[1]
    pieces = (
        lax.all_gather(query_weight, "ep", axis=0, tiled=True),
        lax.all_gather(forget_weight, "ep", axis=0, tiled=True),
        lax.all_gather(input_weight, "ep", axis=0, tiled=True),
    )
    queries, forget_pre, fresh_values = tuple(
        (jnp.dot(normed, weight_rows, preferred_element_type=jnp.float32) for weight_rows in pieces)
    )
    forget = (lower_bound + (1.0 - lower_bound) * jax.nn.sigmoid(forget_pre)).reshape(
        seq_dev, head_count, head_size
    )
    queries = queries.reshape(seq_dev, head_count, head_size)
    fresh_values = fresh_values.reshape(seq_dev, head_count, head_size)
    new_state = forget[..., None] * state + (1.0 - forget)[..., None] * fresh_values[:, :, None, :]
    readout = jnp.einsum("shk,shkv->shv", queries, new_state, precision=lax.Precision.HIGHEST)
    readout = rms_scale(readout, head_gain.reshape(head_count, head_size))
    heads_out = readout.reshape(seq_dev, proj_width).astype(jnp.bfloat16)
    partial_mix = jnp.dot(
        heads_out,
        lax.all_gather(out_weight, "ep", axis=1, tiled=True),
        preferred_element_type=jnp.float32,
    )
    mixer_sum = lax.psum(partial_mix.astype(jnp.bfloat16), "tp").astype(jnp.float32)
    after_mixer = (residual + mixer_sum).astype(jnp.bfloat16)
    ffn_in = rms_scale(after_mixer.astype(jnp.float32), ffn_gain).astype(jnp.bfloat16)
    capacity = 3 * seq_dev // 8
    expert_span = ep_count // EXPERTS
    half_width = model_width // lax.axis_size("tp")
    own_columns = lax.dynamic_slice_in_dim(
        after_mixer, lax.axis_index("tp") * half_width, half_width, 1
    ).astype(jnp.float32)
    gate_slice = expert_gate[0]
    up_slice = expert_up[0]
    down_slice = expert_down[0]
    slot_iota = jnp.arange(capacity, dtype=jnp.int32)
    own_rank = slot_ranks(route_ids.reshape(1, seq_dev * TOP), EXPERTS).reshape(seq_dev, TOP)
    expert_iota = jnp.arange(EXPERTS, dtype=jnp.int32)
    chosen = (route_ids[:, :, None, None] == expert_iota[None, None, :, None]) & (
        own_rank[:, :, None, None] == slot_iota[None, None, None, :]
    )
    dispatch = jnp.any(chosen, axis=1).astype(jnp.bfloat16)
    combine = jnp.sum(chosen.astype(jnp.float32) * route_weights[:, :, None, None], axis=1)
    outgoing = jnp.einsum(
        "tec,td->ecd", dispatch, ffn_in, preferred_element_type=jnp.float32
    ).astype(jnp.bfloat16)
    outgoing = jnp.broadcast_to(
        outgoing[:, None], (EXPERTS, expert_span, capacity, model_width)
    ).reshape(ep_count, capacity, model_width)
    slot_rows = lax.all_to_all(outgoing, "ep", split_axis=0, concat_axis=0, tiled=True)
    gate_pre = jnp.einsum(
        "...d,df->...f", slot_rows, gate_slice, preferred_element_type=jnp.float32
    )
    up_pre = jnp.einsum("...d,df->...f", slot_rows, up_slice, preferred_element_type=jnp.float32)
    hidden = (jax.nn.silu(gate_pre) * up_pre).astype(jnp.bfloat16)
    partial_out = jnp.einsum(
        "...f,fd->...d", hidden, down_slice, preferred_element_type=jnp.float32
    )
    reduced = lax.psum_scatter(
        partial_out.astype(jnp.bfloat16), "tp", scatter_dimension=2, tiled=True
    ).astype(jnp.float32)
    returned = lax.all_to_all(
        reduced.astype(jnp.bfloat16), "ep", split_axis=0, concat_axis=0, tiled=True
    ).astype(reduced.dtype)
    expert_out = jnp.sum(returned.reshape(EXPERTS, expert_span, capacity, half_width), axis=1)
    expert_mix = jnp.einsum("tec,ecd->td", combine, expert_out, precision=lax.Precision.HIGHEST)
    mixed_out = (own_columns + expert_mix).astype(jnp.bfloat16)
    return (mixed_out, new_state)


def layer_kernel(
    n,
    m,
    capacity,
    tokens_ref,
    mix_gain_ref,
    query_ref,
    forget_ref,
    input_ref,
    bound_ref,
    head_gain_ref,
    out_ref,
    state_hbm,
    ffn_gain_ref,
    ids_ref,
    weights_ref,
    gate_hbm,
    up_hbm,
    down_hbm,
    mixed_ref,
    state_buf,
    gate_buf,
    up_buf,
    down_buf,
    x_send,
    x_recv,
    p_send,
    p_recv,
    h_send,
    h_recv,
    m_send,
    m_recv,
    after_buf,
    ffn_buf,
    o_send,
    o_recv,
    hidden_buf,
    c_send,
    c_recv,
    r_send,
    r_recv,
    own_buf,
    local_sem,
    send_sem,
    recv_sem,
    share_sem,
    back_sem,
):
    me = lax.axis_index("ep")
    core = lax.axis_index("tp")
    f32, bf16 = jnp.float32, jnp.bfloat16
    seqs, width = tokens_ref.shape
    rows = query_ref.shape[0]
    proj = query_ref.shape[1]
    heads = state_buf.shape[1]
    size = state_buf.shape[2]
    span = n // EXPERTS
    half = width // m

    loads = [
        pltpu.make_async_copy(state_hbm, state_buf, local_sem.at[0]),
        pltpu.make_async_copy(gate_hbm.at[0], gate_buf, local_sem.at[1]),
        pltpu.make_async_copy(up_hbm.at[0], up_buf, local_sem.at[2]),
        pltpu.make_async_copy(down_hbm.at[0], down_buf, local_sem.at[3]),
    ]
    for load in loads:
        load.start()

    barrier = pltpu.get_barrier_semaphore()
    for shift in range(m):
        other = lax.rem(core + shift, m)

        def greet(i, carry, other=other):
            pl.semaphore_signal(
                barrier, inc=1, device_id=(lax.rem(me + i, n), other), device_id_type=MESH
            )
            return carry

        lax.fori_loop(0 if shift else 1, n, greet, 0)

    def copy_to(phase, i, shift, source, target):
        peer = lax.rem(me + i, n)
        other = lax.rem(core + shift, m)
        return pltpu.make_async_remote_copy(
            src_ref=source(peer, other),
            dst_ref=target(me, core),
            send_sem=send_sem.at[phase * m + shift, peer],
            recv_sem=recv_sem.at[phase * m + core, me],
            device_id=(peer, other),
            device_id_type=MESH,
        )

    def copy_from(phase, i, shift, target):
        peer = lax.rem(me - i + n, n)
        other = lax.rem(core - shift + m, m)
        landing = target(peer, other)
        return peer, other, pltpu.make_async_remote_copy(
            src_ref=landing,
            dst_ref=landing,
            send_sem=send_sem.at[phase * m + shift, peer],
            recv_sem=recv_sem.at[phase * m + other, peer],
            device_id=(lax.rem(me + i, n), lax.rem(core + shift, m)),
            device_id_type=MESH,
        )

    def send_all(phase, shift, source, target):
        def step(i, carry):
            copy_to(phase, i, shift, source, target).start()
            return carry

        lax.fori_loop(0 if shift else 1, n, step, 0)

    def receive_all(phase, shift, target):
        def step(i, carry):
            copy_from(phase, i, shift, target)[2].wait_recv()
            return carry

        lax.fori_loop(0 if shift else 1, n, step, 0)

    def drain(phase, shift, source, target):
        def step(i, carry):
            copy_to(phase, i, shift, source, target).wait_send()
            return carry

        lax.fori_loop(0 if shift else 1, n, step, 0)

    residual = tokens_ref[...].astype(f32)
    normed = rms_scale(residual, mix_gain_ref[...]).astype(bf16)
    for peer in range(n):
        x_send[peer] = normed[:, peer * rows : (peer + 1) * rows]

    ids = ids_ref[...]
    routed = weights_ref[...]
    pad = -(-capacity // 8) * 8
    slots = EXPERTS * pad
    slot = lax.broadcasted_iota(jnp.int32, (slots, seqs), 0)
    first = jnp.where(slot // pad == ids[0:1, :], 1.0, 0.0)
    second = jnp.where(slot // pad == ids[1:2, :], 1.0, 0.0)
    named = first + second
    upper = jnp.where(
        lax.broadcasted_iota(jnp.int32, (seqs, seqs), 0)
        < lax.broadcasted_iota(jnp.int32, (seqs, seqs), 1),
        1.0,
        0.0,
    )
    before = jnp.dot(named.astype(bf16), upper.astype(bf16), preferred_element_type=f32)
    taken = jnp.where(jnp.abs(before - (slot % pad).astype(f32)) < 0.5, named, 0.0)
    combine = (taken * (first * routed[0:1, :] + second * routed[1:2, :])).T

    pl.semaphore_wait(barrier, n * m - 1)

    x_source, x_target = lambda p, c: x_send.at[p], lambda p, c: x_recv.at[p]
    send_all(0, 0, x_source, x_target)
    x_recv[pl.ds(me, 1)] = x_send[pl.ds(me, 1)]
    receive_all(0, 0, x_target)

    gathered = x_recv[...].reshape(n * seqs, rows)
    for part, ref in enumerate((query_ref, forget_ref, input_ref)):
        p_send[:, :, part * proj : (part + 1) * proj] = (
            jnp.dot(gathered, ref[...], preferred_element_type=f32)
            .reshape(n, seqs, proj)
            .astype(bf16)
        )
    p_source, p_target = lambda p, c: p_send.at[p], lambda p, c: p_recv.at[p]
    send_all(1, 0, p_source, p_target)

    def add_part(i, total):
        peer, _, copy = copy_from(1, i, 0, p_target)
        copy.wait_recv()
        return total + p_recv[peer].astype(f32)

    total = lax.fori_loop(1, n, add_part, p_send[me].astype(f32))
    queries = total[:, :proj]
    bound = bound_ref[...]
    forget = bound + (1.0 - bound) * jax.nn.sigmoid(total[:, proj : 2 * proj])
    fresh = total[:, 2 * proj :]

    loads[0].wait()
    scaled = (queries * forget).astype(bf16)
    rest = queries * (1.0 - forget)
    row_of = lax.broadcasted_iota(jnp.int32, (seqs, size), 0)

    def read_row(s, sums):
        return tuple(
            jnp.where(
                row_of == s,
                jnp.dot(
                    scaled[:, h * size : (h + 1) * size],
                    state_buf[s, h].astype(bf16),
                    preferred_element_type=f32,
                ),
                sums[h],
            )
            for h in range(heads)
        )

    sums = lax.fori_loop(
        0, seqs, read_row, tuple(jnp.zeros((seqs, size), f32) for _ in range(heads)), unroll=4
    )
    for h in range(heads):
        cut = slice(h * size, (h + 1) * size)
        readout = sums[h] + jnp.sum(rest[:, cut], axis=-1, keepdims=True) * fresh[:, cut]
        h_send[:, cut] = rms_scale(readout, head_gain_ref[:, cut]).astype(bf16)

    h_source, h_target = lambda p, c: h_send, lambda p, c: h_recv.at[p]
    send_all(2, 0, h_source, h_target)
    h_recv[pl.ds(me, 1)] = h_send[...][None]
    forget_columns = forget.T
    for s in range(seqs):
        for h in range(heads):
            keep = forget_columns[h * size : (h + 1) * size, s : s + 1]
            entering = fresh[s : s + 1, h * size : (h + 1) * size]
            state_buf[s, h] = keep * state_buf[s, h] + (1.0 - keep) * entering
    receive_all(2, 0, h_target)
    m_send[...] = (
        jnp.dot(h_recv[...].reshape(n * seqs, proj), out_ref[...], preferred_element_type=f32)
        .reshape(n, seqs, rows)
        .astype(bf16)
    )
    m_source, m_target = lambda p, c: m_send.at[p], lambda p, c: m_recv.at[c, p]
    for shift in range(m):
        send_all(3, shift, m_source, m_target)
    m_recv[pl.ds(core, 1), pl.ds(me, 1)] = m_send[pl.ds(me, 1)][None]
    for shift in range(m):
        receive_all(3, shift, m_target)
    mixer_sum = jnp.concatenate(
        [sum(m_recv[c, p].astype(f32) for c in range(m)) for p in range(n)], axis=1
    )
    after = (residual + mixer_sum).astype(bf16).astype(f32)
    after_buf[...] = after
    ffn_buf[...] = rms_scale(after, ffn_gain_ref[...]).astype(bf16)
    own_cut = pl.ds(pl.multiple_of(core * half, 128), half)
    o_send[...] = (
        jnp.dot(taken.astype(bf16), ffn_buf[:, own_cut], preferred_element_type=f32)
        .reshape(EXPERTS, pad, half)
        .astype(bf16)
    )
    used = pl.ds(0, capacity)
    o_source = lambda p, c: o_send.at[lax.div(p, span), used]
    o_target = lambda p, c: o_recv.at[c, p, used]
    send_all(4, 0, o_source, o_target)
    o_recv[pl.ds(core, 1), pl.ds(me, 1)] = o_send[pl.ds(lax.div(me, span), 1)][None]

    def share(peer, shift):
        other = lax.rem(core + shift, m)
        block = o_recv.at[core, peer, used]
        return pltpu.make_async_remote_copy(
            src_ref=block,
            dst_ref=block,
            send_sem=send_sem.at[4 * m + shift, peer],
            recv_sem=share_sem.at[core, peer],
            device_id=(me, other),
            device_id_type=MESH,
        )

    def pass_on(i, carry):
        peer, _, copy = copy_from(4, i, 0, o_target)

        @pl.when(i > 0)
        def _():
            copy.wait_recv()

        for shift in range(1, m):
            share(peer, shift).start()
        return carry

    lax.fori_loop(0, n, pass_on, 0)

    def shared(i, carry):
        for shift in range(1, m):
            other = lax.rem(core - shift + m, m)
            block = o_recv.at[other, i, used]
            pltpu.make_async_remote_copy(
                src_ref=block,
                dst_ref=block,
                send_sem=send_sem.at[4 * m + shift, i],
                recv_sem=share_sem.at[other, i],
                device_id=(me, lax.rem(core + shift, m)),
                device_id_type=MESH,
            ).wait_recv()
        return carry

    for load in loads[1:3]:
        load.wait()
    lax.fori_loop(0, n, shared, 0)
    slot_rows = [
        o_recv[c].astype(f32).reshape(n * pad, half).astype(bf16) for c in range(m)
    ]
    tile = 256

    def hidden_step(j, carry):
        cut = pl.ds(pl.multiple_of(j * tile, tile), tile)
        gate_pre, up_pre = (
            sum(
                jnp.dot(
                    slot_rows[c],
                    ref[c * half : (c + 1) * half, cut],
                    preferred_element_type=f32,
                )
                for c in range(m)
            )
            for ref in (gate_buf, up_buf)
        )
        hidden_buf[:, cut] = (jax.nn.silu(gate_pre) * up_pre).astype(bf16)
        return carry

    lax.fori_loop(0, gate_buf.shape[1] // tile, hidden_step, 0)
    hidden = hidden_buf[...]
    loads[3].wait()

    def down_into(side, target):
        def down_step(j, carry):
            cut = pl.ds(pl.multiple_of(j * tile, tile), tile)
            from_cut = pl.ds(pl.multiple_of(side * half + j * tile, tile), tile)
            target[:, :, cut] = (
                jnp.dot(hidden, down_buf[:, from_cut], preferred_element_type=f32)
                .reshape(n, pad, tile)
                .astype(target.dtype)
            )
            return carry

        lax.fori_loop(0, half // tile, down_step, 0)

    def trade(shift):
        return pltpu.make_async_remote_copy(
            src_ref=c_send.at[shift - 1],
            dst_ref=c_recv.at[shift - 1],
            send_sem=send_sem.at[5 * m + shift, 0],
            recv_sem=recv_sem.at[5 * m + shift, 0],
            device_id=(me, lax.rem(core + shift, m)),
            device_id_type=MESH,
        )

    for shift in range(1, m):
        down_into(lax.rem(core + shift, m), c_send.at[shift - 1])
        trade(shift).start()
    down_into(core, own_buf)
    reduced = own_buf[...]
    for shift in range(1, m):
        trade(shift).wait_recv()
        reduced = reduced + c_recv[shift - 1].astype(f32)
    r_send[...] = reduced.astype(bf16)

    def send_back(i, carry):
        copy_back(i).start()
        return carry

    def copy_back(i):
        peer = lax.rem(me + i, n)
        return pltpu.make_async_remote_copy(
            src_ref=r_send.at[peer, used],
            dst_ref=r_recv.at[me, used],
            send_sem=send_sem.at[5 * m, peer],
            recv_sem=back_sem.at[me],
            device_id=(peer, core),
            device_id_type=MESH,
        )

    lax.fori_loop(1, n, send_back, 0)
    r_recv[pl.ds(me, 1)] = r_send[pl.ds(me, 1)]

    def get_back(i, carry):
        peer = lax.rem(me - i + n, n)
        landing = r_recv.at[peer, used]
        pltpu.make_async_remote_copy(
            src_ref=landing,
            dst_ref=landing,
            send_sem=send_sem.at[5 * m, peer],
            recv_sem=back_sem.at[peer],
            device_id=(peer, core),
            device_id_type=MESH,
        ).wait_recv()
        return carry

    lax.fori_loop(1, n, get_back, 0)
    real = lax.broadcasted_iota(jnp.int32, (pad, half), 0) < capacity
    expert_out = jnp.concatenate(
        [
            jnp.where(real, sum(r_recv[e * span + k].astype(f32) for k in range(span)), 0.0)
            for e in range(EXPERTS)
        ],
        axis=0,
    )
    expert_mix = jnp.dot(
        combine, expert_out, preferred_element_type=f32, precision=lax.Precision.HIGHEST
    )
    own = after_buf[:, own_cut]
    mixed_ref[...] = (own + expert_mix).astype(bf16)

    drain(0, 0, x_source, x_target)
    drain(1, 0, p_source, p_target)
    drain(2, 0, h_source, h_target)
    drain(4, 0, o_source, o_target)
    for shift in range(m):
        drain(3, shift, m_source, m_target)

    def drain_rest(i, carry):
        for shift in range(1, m):
            share(i, shift).wait_send()

        @pl.when(i > 0)
        def _():
            copy_back(i).wait_send()

        return carry

    lax.fori_loop(0, n, drain_rest, 0)
    for shift in range(1, m):
        trade(shift).wait_send()


def exchanged_shards(
    n,
    m,
    tokens,
    mix_gain,
    query_weight,
    forget_weight,
    input_weight,
    lower_bound,
    head_gain,
    out_weight,
    state,
    ffn_gain,
    route_ids,
    route_weights,
    expert_gate,
    expert_up,
    expert_down,
):
    seqs, width = tokens.shape
    rows, proj = query_weight.shape
    columns = out_weight.shape[1]
    hidden = expert_gate.shape[2]
    half = width // m
    f32, bf16 = jnp.float32, jnp.bfloat16
    vmem, far = pl.BlockSpec(memory_space=pltpu.VMEM), pl.BlockSpec(memory_space=pltpu.HBM)
    pad = -(-(3 * seqs // 8) // 8) * 8
    mixed_out, new_state = pl.pallas_call(
        functools.partial(layer_kernel, n, m, 3 * seqs // 8),
        out_shape=(
            jax.ShapeDtypeStruct((seqs, half), bf16),
            pltpu.VMEM(state.shape, f32),
        ),
        in_specs=[vmem] * 8 + [far] + [vmem] * 3 + [far] * 3,
        out_specs=(vmem, vmem),
        scratch_shapes=[
            pltpu.VMEM(expert_gate.shape[1:], bf16),
            pltpu.VMEM(expert_up.shape[1:], bf16),
            pltpu.VMEM(expert_down.shape[1:], bf16),
            pltpu.VMEM((n, seqs, rows), bf16),
            pltpu.VMEM((n, seqs, rows), bf16),
            pltpu.VMEM((n, seqs, 3 * proj), bf16),
            pltpu.VMEM((n, seqs, 3 * proj), bf16),
            pltpu.VMEM((seqs, proj), bf16),
            pltpu.VMEM((n, seqs, proj), bf16),
            pltpu.VMEM((n, seqs, columns), bf16),
            pltpu.VMEM((m, n, seqs, columns), bf16),
            pltpu.VMEM((seqs, width), f32),
            pltpu.VMEM((seqs, width), bf16),
            pltpu.VMEM((EXPERTS, pad, half), bf16),
            pltpu.VMEM((m, n, pad, half), bf16),
            pltpu.VMEM((n * pad, hidden), bf16),
            pltpu.VMEM((m - 1, n, pad, half), bf16),
            pltpu.VMEM((m - 1, n, pad, half), bf16),
            pltpu.VMEM((n, pad, half), bf16),
            pltpu.VMEM((n, pad, half), bf16),
            pltpu.VMEM((n, pad, half), f32),
            pltpu.SemaphoreType.DMA((4,)),
            pltpu.SemaphoreType.DMA((6 * m, n)),
            pltpu.SemaphoreType.DMA((6 * m, n)),
            pltpu.SemaphoreType.DMA((m, n)),
            pltpu.SemaphoreType.DMA((n,)),
        ],
        compiler_params=pltpu.CompilerParams(
            collective_id=0, has_side_effects=True, vmem_limit_bytes=60000 * 1024
        ),
    )(
        tokens,
        mix_gain[None],
        query_weight,
        forget_weight,
        input_weight,
        lower_bound[None],
        head_gain[None],
        out_weight,
        state,
        ffn_gain[None],
        route_ids.T,
        route_weights.T,
        expert_gate,
        expert_up,
        expert_down,
    )
    return (mixed_out, new_state)


def solution(mesh):
    n, m = mesh.shape["ep"], mesh.shape["tp"]

    def body(*args):
        rows = args[2].shape[0]
        columns = args[7].shape[1]
        if rows % 128 or columns % 128:
            return gathered_shards(*args)
        return exchanged_shards(n, m, *args)

    return jax.shard_map(
        body,
        mesh=mesh,
        in_specs=(
            P("ep", None),
            P(),
            P("ep", "tp"),
            P("ep", "tp"),
            P("ep", "tp"),
            P("tp"),
            P("tp"),
            P("tp", "ep"),
            P("ep", "tp", None, None),
            P(),
            P("ep", None),
            P("ep", None),
            P("ep", None, "tp"),
            P("ep", None, "tp"),
            P("ep", "tp", None),
        ),
        out_specs=(P("ep", "tp"), P("ep", "tp", None, None)),
        check_vma=False,
    )
```

```python
import functools

import jax
import jax.numpy as jnp
from jax import lax
from jax.experimental import pallas as pl
from jax.experimental.pallas import tpu as pltpu
from jax.sharding import PartitionSpec as P

MESH = pl.DeviceIdType.MESH
PLANE = 4
EXPERTS = 8
TOP = 2


epsilon = 1e-06


def rms_scale(values_in, gain_vec):
    return (
        values_in
        * lax.rsqrt(jnp.mean(values_in * values_in, axis=-1, keepdims=True) + epsilon)
        * gain_vec
    )


def slot_ranks(block_ids, expert_count):
    onehot = (block_ids[..., None] == jnp.arange(expert_count, dtype=jnp.int32)).astype(jnp.int32)
    before = jnp.cumsum(onehot, axis=1) - onehot
    return jnp.sum(before * onehot, axis=-1)


def gathered_shards(
    tokens,
    mix_gain,
    query_weight,
    forget_weight,
    input_weight,
    lower_bound,
    head_gain,
    out_weight,
    state,
    ffn_gain,
    route_ids,
    route_weights,
    expert_gate,
    expert_up,
    expert_down,
):
    seq_dev = tokens.shape[0]
    model_width = tokens.shape[1]
    ep_count = lax.axis_size("ep")
    residual = tokens.astype(jnp.float32)
    normed = rms_scale(residual, mix_gain).astype(jnp.bfloat16)
    head_count = state.shape[1]
    head_size = state.shape[2]
    proj_width = query_weight.shape[1]
    pieces = (
        lax.all_gather(query_weight, "ep", axis=0, tiled=True),
        lax.all_gather(forget_weight, "ep", axis=0, tiled=True),
        lax.all_gather(input_weight, "ep", axis=0, tiled=True),
    )
    queries, forget_pre, fresh_values = tuple(
        (jnp.dot(normed, weight_rows, preferred_element_type=jnp.float32) for weight_rows in pieces)
    )
    forget = (lower_bound + (1.0 - lower_bound) * jax.nn.sigmoid(forget_pre)).reshape(
        seq_dev, head_count, head_size
    )
    queries = queries.reshape(seq_dev, head_count, head_size)
    fresh_values = fresh_values.reshape(seq_dev, head_count, head_size)
    new_state = forget[..., None] * state + (1.0 - forget)[..., None] * fresh_values[:, :, None, :]
    readout = jnp.einsum("shk,shkv->shv", queries, new_state, precision=lax.Precision.HIGHEST)
    readout = rms_scale(readout, head_gain.reshape(head_count, head_size))
    heads_out = readout.reshape(seq_dev, proj_width).astype(jnp.bfloat16)
    partial_mix = jnp.dot(
        heads_out,
        lax.all_gather(out_weight, "ep", axis=1, tiled=True),
        preferred_element_type=jnp.float32,
    )
    mixer_sum = lax.psum(partial_mix.astype(jnp.bfloat16), "tp").astype(jnp.float32)
    after_mixer = (residual + mixer_sum).astype(jnp.bfloat16)
    ffn_in = rms_scale(after_mixer.astype(jnp.float32), ffn_gain).astype(jnp.bfloat16)
    capacity = 3 * seq_dev // 8
    expert_span = ep_count // EXPERTS
    half_width = model_width // lax.axis_size("tp")
    own_columns = lax.dynamic_slice_in_dim(
        after_mixer, lax.axis_index("tp") * half_width, half_width, 1
    ).astype(jnp.float32)
    gate_slice = expert_gate[0]
    up_slice = expert_up[0]
    down_slice = expert_down[0]
    slot_iota = jnp.arange(capacity, dtype=jnp.int32)
    own_rank = slot_ranks(route_ids.reshape(1, seq_dev * TOP), EXPERTS).reshape(seq_dev, TOP)
    expert_iota = jnp.arange(EXPERTS, dtype=jnp.int32)
    chosen = (route_ids[:, :, None, None] == expert_iota[None, None, :, None]) & (
        own_rank[:, :, None, None] == slot_iota[None, None, None, :]
    )
    dispatch = jnp.any(chosen, axis=1).astype(jnp.bfloat16)
    combine = jnp.sum(chosen.astype(jnp.float32) * route_weights[:, :, None, None], axis=1)
    outgoing = jnp.einsum(
        "tec,td->ecd", dispatch, ffn_in, preferred_element_type=jnp.float32
    ).astype(jnp.bfloat16)
    outgoing = jnp.broadcast_to(
        outgoing[:, None], (EXPERTS, expert_span, capacity, model_width)
    ).reshape(ep_count, capacity, model_width)
    slot_rows = lax.all_to_all(outgoing, "ep", split_axis=0, concat_axis=0, tiled=True)
    gate_pre = jnp.einsum(
        "...d,df->...f", slot_rows, gate_slice, preferred_element_type=jnp.float32
    )
    up_pre = jnp.einsum("...d,df->...f", slot_rows, up_slice, preferred_element_type=jnp.float32)
    hidden = (jax.nn.silu(gate_pre) * up_pre).astype(jnp.bfloat16)
    partial_out = jnp.einsum(
        "...f,fd->...d", hidden, down_slice, preferred_element_type=jnp.float32
    )
    reduced = lax.psum_scatter(
        partial_out.astype(jnp.bfloat16), "tp", scatter_dimension=2, tiled=True
    ).astype(jnp.float32)
    returned = lax.all_to_all(
        reduced.astype(jnp.bfloat16), "ep", split_axis=0, concat_axis=0, tiled=True
    ).astype(reduced.dtype)
    expert_out = jnp.sum(returned.reshape(EXPERTS, expert_span, capacity, half_width), axis=1)
    expert_mix = jnp.einsum("tec,ecd->td", combine, expert_out, precision=lax.Precision.HIGHEST)
    mixed_out = (own_columns + expert_mix).astype(jnp.bfloat16)
    return (mixed_out, new_state)


def layer_kernel(
    n,
    m,
    capacity,
    tokens_ref,
    mix_gain_ref,
    query_ref,
    forget_ref,
    input_ref,
    bound_ref,
    head_gain_ref,
    out_ref,
    state_hbm,
    ffn_gain_ref,
    ids_ref,
    weights_ref,
    gate_hbm,
    up_hbm,
    down_hbm,
    mixed_ref,
    state_buf,
    gate_buf,
    up_buf,
    down_buf,
    x_send,
    x_recv,
    p_send,
    p_recv,
    s_send,
    s_recv,
    out_all,
    h_send,
    h_recv,
    m_send,
    m_recv,
    after_buf,
    ffn_buf,
    o_send,
    o_recv,
    hidden_buf,
    c_send,
    c_recv,
    r_send,
    r_recv,
    own_buf,
    local_sem,
    send_sem,
    recv_sem,
    share_sem,
    back_sem,
):
    me = lax.axis_index("ep")
    core = lax.axis_index("tp")
    f32, bf16 = jnp.float32, jnp.bfloat16
    seqs, width = tokens_ref.shape
    rows = query_ref.shape[0]
    proj = query_ref.shape[1]
    heads = state_buf.shape[1]
    size = state_buf.shape[2]
    span = n // EXPERTS
    half = width // m

    loads = [
        pltpu.make_async_copy(state_hbm, state_buf, local_sem.at[0]),
        pltpu.make_async_copy(gate_hbm.at[0], gate_buf, local_sem.at[1]),
        pltpu.make_async_copy(up_hbm.at[0], up_buf, local_sem.at[2]),
        pltpu.make_async_copy(down_hbm.at[0], down_buf, local_sem.at[3]),
    ]
    for load in loads:
        load.start()

    barrier = pltpu.get_barrier_semaphore()
    for shift in range(m):
        other = lax.rem(core + shift, m)

        def greet(i, carry, other=other):
            pl.semaphore_signal(
                barrier, inc=1, device_id=(lax.rem(me + i, n), other), device_id_type=MESH
            )
            return carry

        lax.fori_loop(0 if shift else 1, n, greet, 0)

    plane = PLANE
    lines = n // plane
    level, place = lax.div(me, plane), lax.rem(me, plane)
    counts = {"all": n, "line": lines, "plane": plane}

    def partner(group, i):
        if group == "plane":
            return level * plane + lax.rem(place + i + plane, plane)
        return lax.rem(me + i * (plane if group == "line" else 1) + n, n)

    def copy_to(phase, i, shift, source, target, group="all"):
        peer = partner(group, i)
        other = lax.rem(core + shift, m)
        return pltpu.make_async_remote_copy(
            src_ref=source(peer, other),
            dst_ref=target(me, core),
            send_sem=send_sem.at[phase * m + shift, peer],
            recv_sem=recv_sem.at[phase * m + core, me],
            device_id=(peer, other),
            device_id_type=MESH,
        )

    def copy_from(phase, i, shift, target, group="all"):
        peer = partner(group, -i)
        other = lax.rem(core - shift + m, m)
        landing = target(peer, other)
        return peer, other, pltpu.make_async_remote_copy(
            src_ref=landing,
            dst_ref=landing,
            send_sem=send_sem.at[phase * m + shift, peer],
            recv_sem=recv_sem.at[phase * m + other, peer],
            device_id=(partner(group, i), lax.rem(core + shift, m)),
            device_id_type=MESH,
        )

    def send_all(phase, shift, source, target, group="all"):
        def step(i, carry):
            copy_to(phase, i, shift, source, target, group).start()
            return carry

        lax.fori_loop(0 if shift else 1, counts[group], step, 0)

    def receive_all(phase, shift, target, group="all"):
        def step(i, carry):
            copy_from(phase, i, shift, target, group)[2].wait_recv()
            return carry

        lax.fori_loop(0 if shift else 1, counts[group], step, 0)

    def drain(phase, shift, source, target, group="all"):
        def step(i, carry):
            copy_to(phase, i, shift, source, target, group).wait_send()
            return carry

        lax.fori_loop(0 if shift else 1, counts[group], step, 0)

    residual = tokens_ref[...].astype(f32)
    normed = rms_scale(residual, mix_gain_ref[...]).astype(bf16)
    for peer in range(n):
        x_send[peer] = normed[:, peer * rows : (peer + 1) * rows]

    ids = ids_ref[...]
    routed = weights_ref[...]
    pad = -(-capacity // 8) * 8
    slots = EXPERTS * pad
    slot = lax.broadcasted_iota(jnp.int32, (slots, seqs), 0)
    first = jnp.where(slot // pad == ids[0:1, :], 1.0, 0.0)
    second = jnp.where(slot // pad == ids[1:2, :], 1.0, 0.0)
    named = first + second
    upper = jnp.where(
        lax.broadcasted_iota(jnp.int32, (seqs, seqs), 0)
        < lax.broadcasted_iota(jnp.int32, (seqs, seqs), 1),
        1.0,
        0.0,
    )
    before = jnp.dot(named.astype(bf16), upper.astype(bf16), preferred_element_type=f32)
    taken = jnp.where(jnp.abs(before - (slot % pad).astype(f32)) < 0.5, named, 0.0)
    combine = (taken * (first * routed[0:1, :] + second * routed[1:2, :])).T

    pl.semaphore_wait(barrier, n * m - 1)

    x_source, x_target = lambda p, c: x_send.at[p], lambda p, c: x_recv.at[p]
    send_all(0, 0, x_source, x_target)
    w_source, w_target = lambda p, c: out_ref, lambda p, c: out_all.at[lax.rem(p, plane)]
    send_all(6, 0, w_source, w_target, "plane")
    out_all[pl.ds(place, 1)] = out_ref[...][None]
    x_recv[pl.ds(me, 1)] = x_send[pl.ds(me, 1)]
    receive_all(0, 0, x_target)

    gathered = x_recv[...].reshape(n * seqs, rows)
    parts = (query_ref, forget_ref, input_ref)
    p_source = [lambda p, c, k=k: p_send.at[k, lax.rem(p, plane)] for k in range(3)]
    p_target = [lambda p, c, k=k: p_recv.at[k, lax.rem(p, plane)] for k in range(3)]
    s_source = [lambda p, c, k=k: s_send.at[k, lax.div(p, plane)] for k in range(3)]
    s_target = [lambda p, c, k=k: s_recv.at[k, lax.div(p, plane)] for k in range(3)]
    for k, ref in enumerate(parts):
        product = (
            jnp.dot(gathered, ref[...], preferred_element_type=f32)
            .reshape(lines, plane, seqs, proj)
            .astype(bf16)
        )
        for q in range(plane):
            p_send[k, q] = product[:, q]
        send_all(7 + k, 0, p_source[k], p_target[k], "plane")
    for k in range(3):
        receive_all(7 + k, 0, p_target[k], "plane")
        p_recv[k, pl.ds(place, 1)] = p_send[k, pl.ds(place, 1)]
        s_send[k] = sum(p_recv[k, q].astype(f32) for q in range(plane)).astype(bf16)
        send_all(10 + k, 0, s_source[k], s_target[k], "line")
    joined = []
    for k in range(3):
        receive_all(10 + k, 0, s_target[k], "line")
        s_recv[k, pl.ds(level, 1)] = s_send[k, pl.ds(level, 1)]
        joined.append(sum(s_recv[k, z].astype(f32) for z in range(lines)))
    queries, forget_pre, fresh = joined
    bound = bound_ref[...]
    forget = bound + (1.0 - bound) * jax.nn.sigmoid(forget_pre)

    loads[0].wait()
    scaled = (queries * forget).astype(bf16)
    rest = queries * (1.0 - forget)
    row_of = lax.broadcasted_iota(jnp.int32, (seqs, size), 0)

    def read_row(s, sums):
        return tuple(
            jnp.where(
                row_of == s,
                jnp.dot(
                    scaled[:, h * size : (h + 1) * size],
                    state_buf[s, h].astype(bf16),
                    preferred_element_type=f32,
                ),
                sums[h],
            )
            for h in range(heads)
        )

    sums = lax.fori_loop(
        0, seqs, read_row, tuple(jnp.zeros((seqs, size), f32) for _ in range(heads)), unroll=4
    )
    for h in range(heads):
        cut = slice(h * size, (h + 1) * size)
        readout = sums[h] + jnp.sum(rest[:, cut], axis=-1, keepdims=True) * fresh[:, cut]
        h_send[:, cut] = rms_scale(readout, head_gain_ref[:, cut]).astype(bf16)

    h_source, h_target = lambda p, c: h_send, lambda p, c: h_recv.at[lax.div(p, plane)]
    send_all(2, 0, h_source, h_target, "line")
    h_recv[pl.ds(level, 1)] = h_send[...][None]
    forget_columns = forget.T
    for s in range(seqs):
        for h in range(heads):
            keep = forget_columns[h * size : (h + 1) * size, s : s + 1]
            entering = fresh[s : s + 1, h * size : (h + 1) * size]
            state_buf[s, h] = keep * state_buf[s, h] + (1.0 - keep) * entering
    receive_all(6, 0, w_target, "plane")
    receive_all(2, 0, h_target, "line")
    every_head = h_recv[...].reshape(lines * seqs, proj)
    for q in range(plane):
        m_send[:, q] = (
            jnp.dot(every_head, out_all[q], preferred_element_type=f32)
            .reshape(lines, seqs, rows)
            .astype(bf16)
        )
    m_source = lambda p, c: m_send.at[lax.div(p, plane)]
    m_target = lambda p, c: m_recv.at[c, lax.div(p, plane)]
    for shift in range(m):
        send_all(3, shift, m_source, m_target, "line")
    m_recv[pl.ds(core, 1), pl.ds(level, 1)] = m_send[pl.ds(level, 1)][None]
    for shift in range(m):
        receive_all(3, shift, m_target, "line")
    mixer_sum = jnp.concatenate(
        [
            sum(m_recv[c, z, q].astype(f32) for c in range(m))
            for z in range(lines)
            for q in range(plane)
        ],
        axis=1,
    )
    after = (residual + mixer_sum).astype(bf16).astype(f32)
    after_buf[...] = after
    ffn_buf[...] = rms_scale(after, ffn_gain_ref[...]).astype(bf16)
    own_cut = pl.ds(pl.multiple_of(core * half, 128), half)
    o_send[...] = (
        jnp.dot(taken.astype(bf16), ffn_buf[:, own_cut], preferred_element_type=f32)
        .reshape(EXPERTS, pad, half)
        .astype(bf16)
    )
    used = pl.ds(0, capacity)
    o_source = lambda p, c: o_send.at[lax.div(p, span), used]
    o_target = lambda p, c: o_recv.at[c, p, used]
    send_all(4, 0, o_source, o_target)
    o_recv[pl.ds(core, 1), pl.ds(me, 1)] = o_send[pl.ds(lax.div(me, span), 1)][None]

    def share(peer, shift):
        other = lax.rem(core + shift, m)
        block = o_recv.at[core, peer, used]
        return pltpu.make_async_remote_copy(
            src_ref=block,
            dst_ref=block,
            send_sem=send_sem.at[4 * m + shift, peer],
            recv_sem=share_sem.at[core, peer],
            device_id=(me, other),
            device_id_type=MESH,
        )

    def pass_on(i, carry):
        peer, _, copy = copy_from(4, i, 0, o_target)

        @pl.when(i > 0)
        def _():
            copy.wait_recv()

        for shift in range(1, m):
            share(peer, shift).start()
        return carry

    lax.fori_loop(0, n, pass_on, 0)

    def shared(i, carry):
        for shift in range(1, m):
            other = lax.rem(core - shift + m, m)
            block = o_recv.at[other, i, used]
            pltpu.make_async_remote_copy(
                src_ref=block,
                dst_ref=block,
                send_sem=send_sem.at[4 * m + shift, i],
                recv_sem=share_sem.at[other, i],
                device_id=(me, lax.rem(core + shift, m)),
                device_id_type=MESH,
            ).wait_recv()
        return carry

    for load in loads[1:3]:
        load.wait()
    lax.fori_loop(0, n, shared, 0)
    slot_rows = [
        o_recv[c].astype(f32).reshape(n * pad, half).astype(bf16) for c in range(m)
    ]
    tile = 256

    def hidden_step(j, carry):
        cut = pl.ds(pl.multiple_of(j * tile, tile), tile)
        gate_pre, up_pre = (
            sum(
                jnp.dot(
                    slot_rows[c],
                    ref[c * half : (c + 1) * half, cut],
                    preferred_element_type=f32,
                )
                for c in range(m)
            )
            for ref in (gate_buf, up_buf)
        )
        hidden_buf[:, cut] = (jax.nn.silu(gate_pre) * up_pre).astype(bf16)
        return carry

    lax.fori_loop(0, gate_buf.shape[1] // tile, hidden_step, 0)
    hidden = hidden_buf[...]
    loads[3].wait()

    def down_into(side, target):
        def down_step(j, carry):
            cut = pl.ds(pl.multiple_of(j * tile, tile), tile)
            from_cut = pl.ds(pl.multiple_of(side * half + j * tile, tile), tile)
            target[:, :, cut] = (
                jnp.dot(hidden, down_buf[:, from_cut], preferred_element_type=f32)
                .reshape(n, pad, tile)
                .astype(target.dtype)
            )
            return carry

        lax.fori_loop(0, half // tile, down_step, 0)

    def trade(shift):
        return pltpu.make_async_remote_copy(
            src_ref=c_send.at[shift - 1],
            dst_ref=c_recv.at[shift - 1],
            send_sem=send_sem.at[5 * m + shift, 0],
            recv_sem=recv_sem.at[5 * m + shift, 0],
            device_id=(me, lax.rem(core + shift, m)),
            device_id_type=MESH,
        )

    for shift in range(1, m):
        down_into(lax.rem(core + shift, m), c_send.at[shift - 1])
        trade(shift).start()
    down_into(core, own_buf)
    reduced = own_buf[...]
    for shift in range(1, m):
        trade(shift).wait_recv()
        reduced = reduced + c_recv[shift - 1].astype(f32)
    r_send[...] = reduced.astype(bf16)

    def send_back(i, carry):
        copy_back(i).start()
        return carry

    def copy_back(i):
        peer = lax.rem(me + i, n)
        return pltpu.make_async_remote_copy(
            src_ref=r_send.at[peer, used],
            dst_ref=r_recv.at[me, used],
            send_sem=send_sem.at[5 * m, peer],
            recv_sem=back_sem.at[me],
            device_id=(peer, core),
            device_id_type=MESH,
        )

    lax.fori_loop(1, n, send_back, 0)
    r_recv[pl.ds(me, 1)] = r_send[pl.ds(me, 1)]

    def get_back(i, carry):
        peer = lax.rem(me - i + n, n)
        landing = r_recv.at[peer, used]
        pltpu.make_async_remote_copy(
            src_ref=landing,
            dst_ref=landing,
            send_sem=send_sem.at[5 * m, peer],
            recv_sem=back_sem.at[peer],
            device_id=(peer, core),
            device_id_type=MESH,
        ).wait_recv()
        return carry

    lax.fori_loop(1, n, get_back, 0)
    real = lax.broadcasted_iota(jnp.int32, (pad, half), 0) < capacity
    expert_out = jnp.concatenate(
        [
            jnp.where(real, sum(r_recv[e * span + k].astype(f32) for k in range(span)), 0.0)
            for e in range(EXPERTS)
        ],
        axis=0,
    )
    expert_mix = jnp.dot(
        combine, expert_out, preferred_element_type=f32, precision=lax.Precision.HIGHEST
    )
    own = after_buf[:, own_cut]
    mixed_ref[...] = (own + expert_mix).astype(bf16)

    drain(0, 0, x_source, x_target)
    drain(6, 0, w_source, w_target, "plane")
    for k in range(3):
        drain(7 + k, 0, p_source[k], p_target[k], "plane")
        drain(10 + k, 0, s_source[k], s_target[k], "line")
    drain(2, 0, h_source, h_target, "line")
    drain(4, 0, o_source, o_target)
    for shift in range(m):
        drain(3, shift, m_source, m_target, "line")

    def drain_rest(i, carry):
        for shift in range(1, m):
            share(i, shift).wait_send()

        @pl.when(i > 0)
        def _():
            copy_back(i).wait_send()

        return carry

    lax.fori_loop(0, n, drain_rest, 0)
    for shift in range(1, m):
        trade(shift).wait_send()


def exchanged_shards(
    n,
    m,
    tokens,
    mix_gain,
    query_weight,
    forget_weight,
    input_weight,
    lower_bound,
    head_gain,
    out_weight,
    state,
    ffn_gain,
    route_ids,
    route_weights,
    expert_gate,
    expert_up,
    expert_down,
):
    seqs, width = tokens.shape
    rows, proj = query_weight.shape
    columns = out_weight.shape[1]
    hidden = expert_gate.shape[2]
    half = width // m
    f32, bf16 = jnp.float32, jnp.bfloat16
    vmem, far = pl.BlockSpec(memory_space=pltpu.VMEM), pl.BlockSpec(memory_space=pltpu.HBM)
    lines = n // PLANE
    pad = -(-(3 * seqs // 8) // 8) * 8
    mixed_out, new_state = pl.pallas_call(
        functools.partial(layer_kernel, n, m, 3 * seqs // 8),
        out_shape=(
            jax.ShapeDtypeStruct((seqs, half), bf16),
            pltpu.VMEM(state.shape, f32),
        ),
        in_specs=[vmem] * 8 + [far] + [vmem] * 3 + [far] * 3,
        out_specs=(vmem, vmem),
        scratch_shapes=[
            pltpu.VMEM(expert_gate.shape[1:], bf16),
            pltpu.VMEM(expert_up.shape[1:], bf16),
            pltpu.VMEM(expert_down.shape[1:], bf16),
            pltpu.VMEM((n, seqs, rows), bf16),
            pltpu.VMEM((n, seqs, rows), bf16),
            pltpu.VMEM((3, PLANE, lines, seqs, proj), bf16),
            pltpu.VMEM((3, PLANE, lines, seqs, proj), bf16),
            pltpu.VMEM((3, lines, seqs, proj), bf16),
            pltpu.VMEM((3, lines, seqs, proj), bf16),
            pltpu.VMEM((PLANE, proj, columns), bf16),
            pltpu.VMEM((seqs, proj), bf16),
            pltpu.VMEM((lines, seqs, proj), bf16),
            pltpu.VMEM((lines, PLANE, seqs, columns), bf16),
            pltpu.VMEM((m, lines, PLANE, seqs, columns), bf16),
            pltpu.VMEM((seqs, width), f32),
            pltpu.VMEM((seqs, width), bf16),
            pltpu.VMEM((EXPERTS, pad, half), bf16),
            pltpu.VMEM((m, n, pad, half), bf16),
            pltpu.VMEM((n * pad, hidden), bf16),
            pltpu.VMEM((m - 1, n, pad, half), bf16),
            pltpu.VMEM((m - 1, n, pad, half), bf16),
            pltpu.VMEM((n, pad, half), bf16),
            pltpu.VMEM((n, pad, half), bf16),
            pltpu.VMEM((n, pad, half), f32),
            pltpu.SemaphoreType.DMA((4,)),
            pltpu.SemaphoreType.DMA((13 * m, n)),
            pltpu.SemaphoreType.DMA((13 * m, n)),
            pltpu.SemaphoreType.DMA((m, n)),
            pltpu.SemaphoreType.DMA((n,)),
        ],
        compiler_params=pltpu.CompilerParams(
            collective_id=0, has_side_effects=True, vmem_limit_bytes=60000 * 1024
        ),
    )(
        tokens,
        mix_gain[None],
        query_weight,
        forget_weight,
        input_weight,
        lower_bound[None],
        head_gain[None],
        out_weight,
        state,
        ffn_gain[None],
        route_ids.T,
        route_weights.T,
        expert_gate,
        expert_up,
        expert_down,
    )
    return (mixed_out, new_state)


def solution(mesh):
    n, m = mesh.shape["ep"], mesh.shape["tp"]

    def body(*args):
        rows = args[2].shape[0]
        columns = args[7].shape[1]
        if rows % 128 or columns % 128 or n % PLANE:
            return gathered_shards(*args)
        return exchanged_shards(n, m, *args)

    return jax.shard_map(
        body,
        mesh=mesh,
        in_specs=(
            P("ep", None),
            P(),
            P("ep", "tp"),
            P("ep", "tp"),
            P("ep", "tp"),
            P("tp"),
            P("tp"),
            P("tp", "ep"),
            P("ep", "tp", None, None),
            P(),
            P("ep", None),
            P("ep", None),
            P("ep", None, "tp"),
            P("ep", None, "tp"),
            P("ep", "tp", None),
        ),
        out_specs=(P("ep", "tp"), P("ep", "tp", None, None)),
        check_vma=False,
    )
```

```python
import functools

import jax
import jax.numpy as jnp
from jax import lax
from jax.experimental import pallas as pl
from jax.experimental.pallas import tpu as pltpu
from jax.sharding import PartitionSpec as P

MESH = pl.DeviceIdType.MESH
PLANE = 4
EXPERTS = 8
TOP = 2


epsilon = 1e-06


def rms_scale(values_in, gain_vec):
    return (
        values_in
        * lax.rsqrt(jnp.mean(values_in * values_in, axis=-1, keepdims=True) + epsilon)
        * gain_vec
    )


def slot_ranks(block_ids, expert_count):
    onehot = (block_ids[..., None] == jnp.arange(expert_count, dtype=jnp.int32)).astype(jnp.int32)
    before = jnp.cumsum(onehot, axis=1) - onehot
    return jnp.sum(before * onehot, axis=-1)


def gathered_shards(
    tokens,
    mix_gain,
    query_weight,
    forget_weight,
    input_weight,
    lower_bound,
    head_gain,
    out_weight,
    state,
    ffn_gain,
    route_ids,
    route_weights,
    expert_gate,
    expert_up,
    expert_down,
):
    seq_dev = tokens.shape[0]
    model_width = tokens.shape[1]
    ep_count = lax.axis_size("ep")
    residual = tokens.astype(jnp.float32)
    normed = rms_scale(residual, mix_gain).astype(jnp.bfloat16)
    head_count = state.shape[1]
    head_size = state.shape[2]
    proj_width = query_weight.shape[1]
    pieces = (
        lax.all_gather(query_weight, "ep", axis=0, tiled=True),
        lax.all_gather(forget_weight, "ep", axis=0, tiled=True),
        lax.all_gather(input_weight, "ep", axis=0, tiled=True),
    )
    queries, forget_pre, fresh_values = tuple(
        (jnp.dot(normed, weight_rows, preferred_element_type=jnp.float32) for weight_rows in pieces)
    )
    forget = (lower_bound + (1.0 - lower_bound) * jax.nn.sigmoid(forget_pre)).reshape(
        seq_dev, head_count, head_size
    )
    queries = queries.reshape(seq_dev, head_count, head_size)
    fresh_values = fresh_values.reshape(seq_dev, head_count, head_size)
    new_state = forget[..., None] * state + (1.0 - forget)[..., None] * fresh_values[:, :, None, :]
    readout = jnp.einsum("shk,shkv->shv", queries, new_state, precision=lax.Precision.HIGHEST)
    readout = rms_scale(readout, head_gain.reshape(head_count, head_size))
    heads_out = readout.reshape(seq_dev, proj_width).astype(jnp.bfloat16)
    partial_mix = jnp.dot(
        heads_out,
        lax.all_gather(out_weight, "ep", axis=1, tiled=True),
        preferred_element_type=jnp.float32,
    )
    mixer_sum = lax.psum(partial_mix.astype(jnp.bfloat16), "tp").astype(jnp.float32)
    after_mixer = (residual + mixer_sum).astype(jnp.bfloat16)
    ffn_in = rms_scale(after_mixer.astype(jnp.float32), ffn_gain).astype(jnp.bfloat16)
    capacity = 3 * seq_dev // 8
    expert_span = ep_count // EXPERTS
    half_width = model_width // lax.axis_size("tp")
    own_columns = lax.dynamic_slice_in_dim(
        after_mixer, lax.axis_index("tp") * half_width, half_width, 1
    ).astype(jnp.float32)
    gate_slice = expert_gate[0]
    up_slice = expert_up[0]
    down_slice = expert_down[0]
    slot_iota = jnp.arange(capacity, dtype=jnp.int32)
    own_rank = slot_ranks(route_ids.reshape(1, seq_dev * TOP), EXPERTS).reshape(seq_dev, TOP)
    expert_iota = jnp.arange(EXPERTS, dtype=jnp.int32)
    chosen = (route_ids[:, :, None, None] == expert_iota[None, None, :, None]) & (
        own_rank[:, :, None, None] == slot_iota[None, None, None, :]
    )
    dispatch = jnp.any(chosen, axis=1).astype(jnp.bfloat16)
    combine = jnp.sum(chosen.astype(jnp.float32) * route_weights[:, :, None, None], axis=1)
    outgoing = jnp.einsum(
        "tec,td->ecd", dispatch, ffn_in, preferred_element_type=jnp.float32
    ).astype(jnp.bfloat16)
    outgoing = jnp.broadcast_to(
        outgoing[:, None], (EXPERTS, expert_span, capacity, model_width)
    ).reshape(ep_count, capacity, model_width)
    slot_rows = lax.all_to_all(outgoing, "ep", split_axis=0, concat_axis=0, tiled=True)
    gate_pre = jnp.einsum(
        "...d,df->...f", slot_rows, gate_slice, preferred_element_type=jnp.float32
    )
    up_pre = jnp.einsum("...d,df->...f", slot_rows, up_slice, preferred_element_type=jnp.float32)
    hidden = (jax.nn.silu(gate_pre) * up_pre).astype(jnp.bfloat16)
    partial_out = jnp.einsum(
        "...f,fd->...d", hidden, down_slice, preferred_element_type=jnp.float32
    )
    reduced = lax.psum_scatter(
        partial_out.astype(jnp.bfloat16), "tp", scatter_dimension=2, tiled=True
    ).astype(jnp.float32)
    returned = lax.all_to_all(
        reduced.astype(jnp.bfloat16), "ep", split_axis=0, concat_axis=0, tiled=True
    ).astype(reduced.dtype)
    expert_out = jnp.sum(returned.reshape(EXPERTS, expert_span, capacity, half_width), axis=1)
    expert_mix = jnp.einsum("tec,ecd->td", combine, expert_out, precision=lax.Precision.HIGHEST)
    mixed_out = (own_columns + expert_mix).astype(jnp.bfloat16)
    return (mixed_out, new_state)


def layer_kernel(
    n,
    m,
    capacity,
    tokens_ref,
    mix_gain_ref,
    query_ref,
    forget_ref,
    input_ref,
    bound_ref,
    head_gain_ref,
    out_ref,
    state_hbm,
    ffn_gain_ref,
    ids_ref,
    weights_ref,
    gate_hbm,
    up_hbm,
    down_hbm,
    mixed_ref,
    state_buf,
    gate_buf,
    up_buf,
    down_buf,
    x_send,
    x_recv,
    p_send,
    p_recv,
    s_send,
    s_recv,
    out_all,
    h_send,
    h_recv,
    m_send,
    m_recv,
    after_buf,
    ffn_buf,
    o_send,
    o_recv,
    hidden_buf,
    c_send,
    c_recv,
    r_send,
    r_recv,
    own_buf,
    local_sem,
    send_sem,
    recv_sem,
    share_sem,
    back_sem,
):
    me = lax.axis_index("ep")
    core = lax.axis_index("tp")
    f32, bf16 = jnp.float32, jnp.bfloat16
    seqs, width = tokens_ref.shape
    rows = query_ref.shape[0]
    proj = query_ref.shape[1]
    heads = state_buf.shape[1]
    size = state_buf.shape[2]
    span = n // EXPERTS
    half = width // m

    loads = [
        pltpu.make_async_copy(state_hbm, state_buf, local_sem.at[0]),
        pltpu.make_async_copy(gate_hbm.at[0], gate_buf, local_sem.at[1]),
        pltpu.make_async_copy(up_hbm.at[0], up_buf, local_sem.at[2]),
        pltpu.make_async_copy(down_hbm.at[0], down_buf, local_sem.at[3]),
    ]
    for load in loads:
        load.start()

    barrier = pltpu.get_barrier_semaphore()
    for shift in range(m):
        other = lax.rem(core + shift, m)

        def greet(i, carry, other=other):
            pl.semaphore_signal(
                barrier, inc=1, device_id=(lax.rem(me + i, n), other), device_id_type=MESH
            )
            return carry

        lax.fori_loop(0 if shift else 1, n, greet, 0)

    plane = PLANE
    lines = n // plane
    level, place = lax.div(me, plane), lax.rem(me, plane)
    counts = {"all": n, "line": lines, "plane": plane}

    def partner(group, i):
        if group == "plane":
            return level * plane + lax.rem(place + i + plane, plane)
        return lax.rem(me + i * (plane if group == "line" else 1) + n, n)

    def copy_to(phase, i, shift, source, target, group="all"):
        peer = partner(group, i)
        other = lax.rem(core + shift, m)
        return pltpu.make_async_remote_copy(
            src_ref=source(peer, other),
            dst_ref=target(me, core),
            send_sem=send_sem.at[phase * m + shift, peer],
            recv_sem=recv_sem.at[phase * m + core, me],
            device_id=(peer, other),
            device_id_type=MESH,
        )

    def copy_from(phase, i, shift, target, group="all"):
        peer = partner(group, -i)
        other = lax.rem(core - shift + m, m)
        landing = target(peer, other)
        return peer, other, pltpu.make_async_remote_copy(
            src_ref=landing,
            dst_ref=landing,
            send_sem=send_sem.at[phase * m + shift, peer],
            recv_sem=recv_sem.at[phase * m + other, peer],
            device_id=(partner(group, i), lax.rem(core + shift, m)),
            device_id_type=MESH,
        )

    def send_all(phase, shift, source, target, group="all"):
        def step(i, carry):
            copy_to(phase, i, shift, source, target, group).start()
            return carry

        lax.fori_loop(0 if shift else 1, counts[group], step, 0)

    def receive_all(phase, shift, target, group="all"):
        def step(i, carry):
            copy_from(phase, i, shift, target, group)[2].wait_recv()
            return carry

        lax.fori_loop(0 if shift else 1, counts[group], step, 0)

    def drain(phase, shift, source, target, group="all"):
        def step(i, carry):
            copy_to(phase, i, shift, source, target, group).wait_send()
            return carry

        lax.fori_loop(0 if shift else 1, counts[group], step, 0)

    residual = tokens_ref[...].astype(f32)
    normed = rms_scale(residual, mix_gain_ref[...]).astype(bf16)
    for peer in range(n):
        x_send[peer] = normed[:, peer * rows : (peer + 1) * rows]

    ids = ids_ref[...]
    routed = weights_ref[...]
    pad = -(-capacity // 8) * 8
    slots = EXPERTS * pad
    slot = lax.broadcasted_iota(jnp.int32, (slots, seqs), 0)
    first = jnp.where(slot // pad == ids[0:1, :], 1.0, 0.0)
    second = jnp.where(slot // pad == ids[1:2, :], 1.0, 0.0)
    named = first + second
    upper = jnp.where(
        lax.broadcasted_iota(jnp.int32, (seqs, seqs), 0)
        < lax.broadcasted_iota(jnp.int32, (seqs, seqs), 1),
        1.0,
        0.0,
    )
    before = jnp.dot(named.astype(bf16), upper.astype(bf16), preferred_element_type=f32)
    taken = jnp.where(jnp.abs(before - (slot % pad).astype(f32)) < 0.5, named, 0.0)
    combine = (taken * (first * routed[0:1, :] + second * routed[1:2, :])).T

    pl.semaphore_wait(barrier, n * m - 1)

    x_source, x_target = lambda p, c: x_send.at[p], lambda p, c: x_recv.at[p]
    send_all(0, 0, x_source, x_target)
    w_source, w_target = lambda p, c: out_ref, lambda p, c: out_all.at[lax.rem(p, plane)]
    out_all[pl.ds(place, 1)] = out_ref[...][None]
    x_recv[pl.ds(me, 1)] = x_send[pl.ds(me, 1)]
    receive_all(0, 0, x_target)

    gathered = x_recv[...].reshape(n * seqs, rows)
    parts = (query_ref, forget_ref, input_ref)
    p_source = [lambda p, c, k=k: p_send.at[k, lax.rem(p, plane)] for k in range(3)]
    p_target = [lambda p, c, k=k: p_recv.at[k, lax.rem(p, plane)] for k in range(3)]
    s_source = [lambda p, c, k=k: s_send.at[k, lax.div(p, plane)] for k in range(3)]
    s_target = [lambda p, c, k=k: s_recv.at[k, lax.div(p, plane)] for k in range(3)]
    for k, ref in enumerate(parts):
        product = (
            jnp.dot(gathered, ref[...], preferred_element_type=f32)
            .reshape(lines, plane, seqs, proj)
            .astype(bf16)
        )
        for q in range(plane):
            p_send[k, q] = product[:, q]
        send_all(7 + k, 0, p_source[k], p_target[k], "plane")
    for k in range(3):
        receive_all(7 + k, 0, p_target[k], "plane")
        p_recv[k, pl.ds(place, 1)] = p_send[k, pl.ds(place, 1)]
        s_send[k] = sum(p_recv[k, q].astype(f32) for q in range(plane)).astype(bf16)
        send_all(10 + k, 0, s_source[k], s_target[k], "line")
    send_all(6, 0, w_source, w_target, "plane")
    joined = []
    for k in range(3):
        receive_all(10 + k, 0, s_target[k], "line")
        s_recv[k, pl.ds(level, 1)] = s_send[k, pl.ds(level, 1)]
        joined.append(sum(s_recv[k, z].astype(f32) for z in range(lines)))
    queries, forget_pre, fresh = joined
    bound = bound_ref[...]
    forget = bound + (1.0 - bound) * jax.nn.sigmoid(forget_pre)

    loads[0].wait()
    scaled = (queries * forget).astype(bf16)
    rest = queries * (1.0 - forget)
    row_of = lax.broadcasted_iota(jnp.int32, (seqs, size), 0)

    def read_row(s, sums):
        return tuple(
            jnp.where(
                row_of == s,
                jnp.dot(
                    scaled[:, h * size : (h + 1) * size],
                    state_buf[s, h].astype(bf16),
                    preferred_element_type=f32,
                ),
                sums[h],
            )
            for h in range(heads)
        )

    sums = lax.fori_loop(
        0, seqs, read_row, tuple(jnp.zeros((seqs, size), f32) for _ in range(heads)), unroll=4
    )
    for h in range(heads):
        cut = slice(h * size, (h + 1) * size)
        readout = sums[h] + jnp.sum(rest[:, cut], axis=-1, keepdims=True) * fresh[:, cut]
        h_send[:, cut] = rms_scale(readout, head_gain_ref[:, cut]).astype(bf16)

    h_source, h_target = lambda p, c: h_send, lambda p, c: h_recv.at[lax.div(p, plane)]
    send_all(2, 0, h_source, h_target, "line")
    h_recv[pl.ds(level, 1)] = h_send[...][None]
    forget_columns = forget.T
    for s in range(seqs):
        for h in range(heads):
            keep = forget_columns[h * size : (h + 1) * size, s : s + 1]
            entering = fresh[s : s + 1, h * size : (h + 1) * size]
            state_buf[s, h] = keep * state_buf[s, h] + (1.0 - keep) * entering
    receive_all(6, 0, w_target, "plane")
    receive_all(2, 0, h_target, "line")
    every_head = h_recv[...].reshape(lines * seqs, proj)
    for q in range(plane):
        m_send[:, q] = (
            jnp.dot(every_head, out_all[q], preferred_element_type=f32)
            .reshape(lines, seqs, rows)
            .astype(bf16)
        )
    m_source = lambda p, c: m_send.at[lax.div(p, plane)]
    m_target = lambda p, c: m_recv.at[c, lax.div(p, plane)]
    for shift in range(m):
        send_all(3, shift, m_source, m_target, "line")
    m_recv[pl.ds(core, 1), pl.ds(level, 1)] = m_send[pl.ds(level, 1)][None]
    for shift in range(m):
        receive_all(3, shift, m_target, "line")
    mixer_sum = jnp.concatenate(
        [
            sum(m_recv[c, z, q].astype(f32) for c in range(m))
            for z in range(lines)
            for q in range(plane)
        ],
        axis=1,
    )
    after = (residual + mixer_sum).astype(bf16).astype(f32)
    after_buf[...] = after
    ffn_buf[...] = rms_scale(after, ffn_gain_ref[...]).astype(bf16)
    own_cut = pl.ds(pl.multiple_of(core * half, 128), half)
    o_send[...] = (
        jnp.dot(taken.astype(bf16), ffn_buf[:, own_cut], preferred_element_type=f32)
        .reshape(EXPERTS, pad, half)
        .astype(bf16)
    )
    used = pl.ds(0, capacity)
    o_source = lambda p, c: o_send.at[lax.div(p, span), used]
    o_target = lambda p, c: o_recv.at[c, p, used]
    send_all(4, 0, o_source, o_target)
    o_recv[pl.ds(core, 1), pl.ds(me, 1)] = o_send[pl.ds(lax.div(me, span), 1)][None]

    def share(peer, shift):
        other = lax.rem(core + shift, m)
        block = o_recv.at[core, peer, used]
        return pltpu.make_async_remote_copy(
            src_ref=block,
            dst_ref=block,
            send_sem=send_sem.at[4 * m + shift, peer],
            recv_sem=share_sem.at[core, peer],
            device_id=(me, other),
            device_id_type=MESH,
        )

    def pass_on(i, carry):
        peer, _, copy = copy_from(4, i, 0, o_target)

        @pl.when(i > 0)
        def _():
            copy.wait_recv()

        for shift in range(1, m):
            share(peer, shift).start()
        return carry

    lax.fori_loop(0, n, pass_on, 0)

    def shared(i, carry):
        for shift in range(1, m):
            other = lax.rem(core - shift + m, m)
            block = o_recv.at[other, i, used]
            pltpu.make_async_remote_copy(
                src_ref=block,
                dst_ref=block,
                send_sem=send_sem.at[4 * m + shift, i],
                recv_sem=share_sem.at[other, i],
                device_id=(me, lax.rem(core + shift, m)),
                device_id_type=MESH,
            ).wait_recv()
        return carry

    for load in loads[1:3]:
        load.wait()
    lax.fori_loop(0, n, shared, 0)
    slot_rows = [
        o_recv[c].astype(f32).reshape(n * pad, half).astype(bf16) for c in range(m)
    ]
    tile = 256

    def hidden_step(j, carry):
        cut = pl.ds(pl.multiple_of(j * tile, tile), tile)
        gate_pre, up_pre = (
            sum(
                jnp.dot(
                    slot_rows[c],
                    ref[c * half : (c + 1) * half, cut],
                    preferred_element_type=f32,
                )
                for c in range(m)
            )
            for ref in (gate_buf, up_buf)
        )
        hidden_buf[:, cut] = (jax.nn.silu(gate_pre) * up_pre).astype(bf16)
        return carry

    lax.fori_loop(0, gate_buf.shape[1] // tile, hidden_step, 0)
    hidden = hidden_buf[...]
    loads[3].wait()

    def down_into(side, target):
        def down_step(j, carry):
            cut = pl.ds(pl.multiple_of(j * tile, tile), tile)
            from_cut = pl.ds(pl.multiple_of(side * half + j * tile, tile), tile)
            target[:, :, cut] = (
                jnp.dot(hidden, down_buf[:, from_cut], preferred_element_type=f32)
                .reshape(n, pad, tile)
                .astype(target.dtype)
            )
            return carry

        lax.fori_loop(0, half // tile, down_step, 0)

    def trade(shift):
        return pltpu.make_async_remote_copy(
            src_ref=c_send.at[shift - 1],
            dst_ref=c_recv.at[shift - 1],
            send_sem=send_sem.at[5 * m + shift, 0],
            recv_sem=recv_sem.at[5 * m + shift, 0],
            device_id=(me, lax.rem(core + shift, m)),
            device_id_type=MESH,
        )

    for shift in range(1, m):
        down_into(lax.rem(core + shift, m), c_send.at[shift - 1])
        trade(shift).start()
    down_into(core, own_buf)
    reduced = own_buf[...]
    for shift in range(1, m):
        trade(shift).wait_recv()
        reduced = reduced + c_recv[shift - 1].astype(f32)
    r_send[...] = reduced.astype(bf16)

    def send_back(i, carry):
        copy_back(i).start()
        return carry

    def copy_back(i):
        peer = lax.rem(me + i, n)
        return pltpu.make_async_remote_copy(
            src_ref=r_send.at[peer, used],
            dst_ref=r_recv.at[me, used],
            send_sem=send_sem.at[5 * m, peer],
            recv_sem=back_sem.at[me],
            device_id=(peer, core),
            device_id_type=MESH,
        )

    lax.fori_loop(1, n, send_back, 0)
    r_recv[pl.ds(me, 1)] = r_send[pl.ds(me, 1)]

    def get_back(i, carry):
        peer = lax.rem(me - i + n, n)
        landing = r_recv.at[peer, used]
        pltpu.make_async_remote_copy(
            src_ref=landing,
            dst_ref=landing,
            send_sem=send_sem.at[5 * m, peer],
            recv_sem=back_sem.at[peer],
            device_id=(peer, core),
            device_id_type=MESH,
        ).wait_recv()
        return carry

    lax.fori_loop(1, n, get_back, 0)
    real = lax.broadcasted_iota(jnp.int32, (pad, half), 0) < capacity
    expert_out = jnp.concatenate(
        [
            jnp.where(real, sum(r_recv[e * span + k].astype(f32) for k in range(span)), 0.0)
            for e in range(EXPERTS)
        ],
        axis=0,
    )
    expert_mix = jnp.dot(
        combine, expert_out, preferred_element_type=f32, precision=lax.Precision.HIGHEST
    )
    own = after_buf[:, own_cut]
    mixed_ref[...] = (own + expert_mix).astype(bf16)

    drain(0, 0, x_source, x_target)
    drain(6, 0, w_source, w_target, "plane")
    for k in range(3):
        drain(7 + k, 0, p_source[k], p_target[k], "plane")
        drain(10 + k, 0, s_source[k], s_target[k], "line")
    drain(2, 0, h_source, h_target, "line")
    drain(4, 0, o_source, o_target)
    for shift in range(m):
        drain(3, shift, m_source, m_target, "line")

    def drain_rest(i, carry):
        for shift in range(1, m):
            share(i, shift).wait_send()

        @pl.when(i > 0)
        def _():
            copy_back(i).wait_send()

        return carry

    lax.fori_loop(0, n, drain_rest, 0)
    for shift in range(1, m):
        trade(shift).wait_send()


def exchanged_shards(
    n,
    m,
    tokens,
    mix_gain,
    query_weight,
    forget_weight,
    input_weight,
    lower_bound,
    head_gain,
    out_weight,
    state,
    ffn_gain,
    route_ids,
    route_weights,
    expert_gate,
    expert_up,
    expert_down,
):
    seqs, width = tokens.shape
    rows, proj = query_weight.shape
    columns = out_weight.shape[1]
    hidden = expert_gate.shape[2]
    half = width // m
    f32, bf16 = jnp.float32, jnp.bfloat16
    vmem, far = pl.BlockSpec(memory_space=pltpu.VMEM), pl.BlockSpec(memory_space=pltpu.HBM)
    lines = n // PLANE
    pad = -(-(3 * seqs // 8) // 8) * 8
    mixed_out, new_state = pl.pallas_call(
        functools.partial(layer_kernel, n, m, 3 * seqs // 8),
        out_shape=(
            jax.ShapeDtypeStruct((seqs, half), bf16),
            pltpu.VMEM(state.shape, f32),
        ),
        in_specs=[vmem] * 8 + [far] + [vmem] * 3 + [far] * 3,
        out_specs=(vmem, vmem),
        scratch_shapes=[
            pltpu.VMEM(expert_gate.shape[1:], bf16),
            pltpu.VMEM(expert_up.shape[1:], bf16),
            pltpu.VMEM(expert_down.shape[1:], bf16),
            pltpu.VMEM((n, seqs, rows), bf16),
            pltpu.VMEM((n, seqs, rows), bf16),
            pltpu.VMEM((3, PLANE, lines, seqs, proj), bf16),
            pltpu.VMEM((3, PLANE, lines, seqs, proj), bf16),
            pltpu.VMEM((3, lines, seqs, proj), bf16),
            pltpu.VMEM((3, lines, seqs, proj), bf16),
            pltpu.VMEM((PLANE, proj, columns), bf16),
            pltpu.VMEM((seqs, proj), bf16),
            pltpu.VMEM((lines, seqs, proj), bf16),
            pltpu.VMEM((lines, PLANE, seqs, columns), bf16),
            pltpu.VMEM((m, lines, PLANE, seqs, columns), bf16),
            pltpu.VMEM((seqs, width), f32),
            pltpu.VMEM((seqs, width), bf16),
            pltpu.VMEM((EXPERTS, pad, half), bf16),
            pltpu.VMEM((m, n, pad, half), bf16),
            pltpu.VMEM((n * pad, hidden), bf16),
            pltpu.VMEM((m - 1, n, pad, half), bf16),
            pltpu.VMEM((m - 1, n, pad, half), bf16),
            pltpu.VMEM((n, pad, half), bf16),
            pltpu.VMEM((n, pad, half), bf16),
            pltpu.VMEM((n, pad, half), f32),
            pltpu.SemaphoreType.DMA((4,)),
            pltpu.SemaphoreType.DMA((13 * m, n)),
            pltpu.SemaphoreType.DMA((13 * m, n)),
            pltpu.SemaphoreType.DMA((m, n)),
            pltpu.SemaphoreType.DMA((n,)),
        ],
        compiler_params=pltpu.CompilerParams(
            collective_id=0, has_side_effects=True, vmem_limit_bytes=60000 * 1024
        ),
    )(
        tokens,
        mix_gain[None],
        query_weight,
        forget_weight,
        input_weight,
        lower_bound[None],
        head_gain[None],
        out_weight,
        state,
        ffn_gain[None],
        route_ids.T,
        route_weights.T,
        expert_gate,
        expert_up,
        expert_down,
    )
    return (mixed_out, new_state)


def solution(mesh):
    n, m = mesh.shape["ep"], mesh.shape["tp"]

    def body(*args):
        rows = args[2].shape[0]
        columns = args[7].shape[1]
        if rows % 128 or columns % 128 or n % PLANE:
            return gathered_shards(*args)
        return exchanged_shards(n, m, *args)

    return jax.shard_map(
        body,
        mesh=mesh,
        in_specs=(
            P("ep", None),
            P(),
            P("ep", "tp"),
            P("ep", "tp"),
            P("ep", "tp"),
            P("tp"),
            P("tp"),
            P("tp", "ep"),
            P("ep", "tp", None, None),
            P(),
            P("ep", None),
            P("ep", None),
            P("ep", None, "tp"),
            P("ep", None, "tp"),
            P("ep", "tp", None),
        ),
        out_specs=(P("ep", "tp"), P("ep", "tp", None, None)),
        check_vma=False,
    )
```
